128 devices in a mesh: gr: 2 (over z_hi), fs: 32 (over z_lo, y, x), tp: 2 (over core).
Axes of the slice: x: 4, y: 4, z: 4 (z_hi: 2, z_lo: 2; z = z_hi * 2 + z_lo), core: 2. Of those that a mesh axis runs over, the one named last changes fastest.
Arguments:
- tokens: bfloat16 [4, 2048, 2048], P(('gr', 'tp')), may hold values from -6 to 6
- gate_master: float32 [3, 2048, 7168], P(None, 'fs', ('gr', 'tp')), may hold values from -0.125 to 0.125
- up_master: float32 [3, 2048, 7168], P(None, 'fs', ('gr', 'tp')), may hold values from -0.125 to 0.125
- down_master: float32 [3, 7168, 2048], P(None, 'fs', ('gr', 'tp')), may hold values from -0.0625 to 0.0625
- norm_gain: float32 [2048], P('fs'), may hold values from 0.1 to 1.9
- route: int32 [4, 2048, 2], P(('gr', 'tp')), may hold values from 0 to 2, all different within a row
- route_weight: float32 [4, 2048, 2], P(('gr', 'tp')), may hold values from 0.05 to 1
Outputs:
- gate_out: bfloat16 [3, 2048, 7168], P(None, None, 'fs')
- up_out: bfloat16 [3, 2048, 7168], P(None, None, 'fs')
- down_out: bfloat16 [3, 7168, 2048], P(None, 'fs')
- mixed: bfloat16 [4, 2048, 2048], P(('gr', 'tp'), 'fs')
The draws below stay inside these ranges and needn't reach their ends.
Inputs may be any that keep to these rules, and one draw needn't show every extreme that they name: `route`: each token names two different experts; every expert is named by some token.
All inputs are finite; a program needn't handle non-finite values.
Results may differ from the reference program's by a relative error of at most 0.024.
Values may be sent and summed in bfloat16 or wider, within the bound.
No kernel may reach another device: no remote copies, remote signals or barrier semaphores. Data moves between devices by JAX's collectives and lax.ppermute only.
A program may use at most 192 MiB of HBM per device.

```python
import math
import jax
import jax.numpy as jnp
from jax import lax

D = 2048
FF = 7168
EXPERTS = 3
ROWS = 2048
REQ = 4
N_FS = 32


def steps_of(rng, shape, shards, low, largest):
    level, own = 1.0, jax.random.fold_in(rng, 6)
    for position, blocks in shards:
        heights = jnp.exp(jax.random.uniform(jax.random.fold_in(own, position), (blocks,), jnp.float32, low / len(shards), largest / len(shards)))
        level = level * jnp.repeat(heights, shape[position] // blocks).reshape([-1 if axis == position else 1 for axis in range(len(shape))])
    return level


def choose_distinct(rng, rows, number_of, top, lift):
    sequence = jax.random.permutation(jax.random.fold_in(rng, 1), number_of)
    boost = sequence
    for power in range(3):
        boost = boost * boost // number_of
    boost = boost * lift // number_of
    lots = jax.random.randint(jax.random.fold_in(rng, 2), (rows, number_of), 0, 4096) + boost
    holders = jax.random.permutation(jax.random.fold_in(rng, 3), rows)[jnp.arange(number_of) % rows]
    lots = jnp.where(jnp.arange(rows)[:, None] == holders[None, :], 1 << 14, lots)
    score = lots * number_of + jnp.arange(number_of)
    return lax.top_k(score.astype(jnp.int32), top)[1].astype(jnp.int32)


def gaussian(own_key, dims, spread, bound, split=(), held_as=jnp.bfloat16):
    values = jax.random.normal(own_key, dims, jnp.float32) * spread
    if len(split) > 0:
        values = steps_of(own_key, dims, split, -0.22, 0.18) * values
    return jnp.clip(values, min=-bound, max=bound).astype(held_as)


def setup_inputs(seed: int = 0) -> dict:
    seeds = jax.random.split(jax.random.key(seed), 8)
    tokens = gaussian(seeds[0], (REQ, ROWS, D), 1.0, 6.0, ((0, 4),))
    gate_master = gaussian(seeds[1], (EXPERTS, D, FF), D ** -0.5, 0.125, ((1, 32), (2, 4)), jnp.float32)
    up_master = gaussian(seeds[2], (EXPERTS, D, FF), D ** -0.5, 0.125, ((1, 32), (2, 4)), jnp.float32)
    down_master = gaussian(seeds[3], (EXPERTS, FF, D), FF ** -0.5, 0.0625, ((1, 32), (2, 4)), jnp.float32)
    norm_gain = jnp.clip(1.0 + 0.18 * jax.random.normal(seeds[4], (D,), jnp.float32), 0.1, 1.9)
    route = choose_distinct(seeds[5], REQ * ROWS, EXPERTS, 2, 0).reshape((REQ, ROWS, 2))
    route_weight = jnp.clip(jnp.exp(math.log(1.0) - 2.9957323 * jax.random.uniform(seeds[6], (REQ, ROWS, 2), jnp.float32) ** steps_of(seeds[6], (REQ, ROWS, 2), ((0, 4),), -0.2, 0.2)), 0.05, 1.0)
    return {"tokens": tokens, "gate_master": gate_master, "up_master": up_master, "down_master": down_master, "norm_gain": norm_gain, "route": route, "route_weight": route_weight}


def normalize(rows_in):
    values = rows_in.astype(jnp.float32)
    scaled = values * lax.rsqrt(lax.optimization_barrier(jnp.mean(values * values, axis=-1, keepdims=True)) + 1e-06)
    return scaled.astype(jnp.bfloat16)

def mixing(chosen, weights):
    share = weights / lax.optimization_barrier(jnp.sum(weights, axis=-1, keepdims=True))
    labels = jnp.arange(EXPERTS, dtype=jnp.int32)
    match = (chosen[:, :, None] == labels[None, None, :]).astype(jnp.float32)
    return lax.optimization_barrier(jnp.sum(share[:, :, None] * match, axis=1))

def reference(tokens, gate_master, up_master, down_master, norm_gain, route, route_weight):
    scaled_gain = norm_gain[None, :, None]
    gate_out = (scaled_gain * gate_master).astype(jnp.bfloat16)
    up_out = (scaled_gain * up_master).astype(jnp.bfloat16)
    down_out = down_master.astype(jnp.bfloat16)
    block_width = FF // N_FS

    def one_batch(batch):
        rows_in, chosen, weights = batch
        normed = normalize(rows_in)
        combine = mixing(chosen, weights)
        hidden_list = []
        for index in range(EXPERTS):
            gate_act = jnp.dot(normed, gate_out[index], preferred_element_type=jnp.float32)
            up_act = jnp.dot(normed, up_out[index], preferred_element_type=jnp.float32)
            hidden_list.append((jax.nn.silu(gate_act) * up_act).astype(jnp.bfloat16))

        def add_block(block, total):
            start = (block * block_width).astype(jnp.int32)
            partial_sum = jnp.zeros((rows_in.shape[0], rows_in.shape[1]), jnp.float32)
            for index in range(EXPERTS):
                hidden_part = lax.dynamic_slice_in_dim(hidden_list[index], start, block_width, 1)
                down_part = lax.dynamic_slice_in_dim(down_out[index], start, block_width, 0)
                projected = jnp.dot(hidden_part, down_part, preferred_element_type=jnp.float32)
                partial_sum = partial_sum + combine[:, index:index + 1] * projected
            return total + partial_sum.astype(jnp.bfloat16).astype(jnp.float32)
        total = lax.fori_loop(0, N_FS, add_block, jnp.zeros((rows_in.shape[0], rows_in.shape[1]), jnp.float32))
        return total.astype(jnp.bfloat16)
    mixed = lax.map(one_batch, (tokens, route, route_weight))
    return (gate_out, up_out, down_out, mixed)
```

```python
import functools

import jax
import jax.numpy as jnp
from jax import lax
from jax.experimental import pallas as pl
from jax.experimental.pallas import tpu as pltpu
from jax.sharding import Mesh
from jax.sharding import PartitionSpec as P

FS = ("fs_0", "fs_1", "fs_2")
Z = ("gr", "fs_0")
VMEM = pl.BlockSpec(memory_space=pltpu.VMEM)
SMEM = pl.BlockSpec(memory_space=pltpu.SMEM)


CHUNKS = (("y", 1), ("x", 1), ("y", 3), ("x", 3))


def cost(flops, nbytes):
    return pl.CostEstimate(flops=int(flops), bytes_accessed=int(nbytes), transcendentals=0)


def params(**kw):
    return pltpu.CompilerParams(vmem_limit_bytes=60 * 1024 * 1024, **kw)


def pack_kernel(where_ref, gate_ref, up_ref, gain_ref, own_ref, send_ref):
    gain = gain_ref[...]
    rows = jnp.concatenate([gate_ref[0] * gain, up_ref[0] * gain], axis=0)
    cols = rows.T.astype(jnp.bfloat16)
    dests, _, half, lanes = own_ref.shape
    cols = cols.reshape(dests, 2, half, lanes)
    low, high = cols[:, 0], cols[:, 1]
    first = where_ref[1] == 0
    own_ref[:, 0] = jnp.where(first, low, high)
    send_ref[:, 0] = jnp.where(first, high, low)


def pack(where, gate, up, gain, dests):
    experts, depth, width = gate.shape
    half = width // dests // 2
    out = jax.ShapeDtypeStruct((dests, experts, half, 2 * depth), jnp.bfloat16)
    spec_in = pl.BlockSpec((1, depth, width), lambda e, w: (e, 0, 0))
    spec_out = pl.BlockSpec((dests, 1, half, 2 * depth), lambda e, w: (0, e, 0, 0))
    return pl.pallas_call(
        pack_kernel,
        out_shape=(out, out),
        grid_spec=pltpu.PrefetchScalarGridSpec(
            num_scalar_prefetch=1,
            grid=(experts,),
            in_specs=[spec_in, spec_in, pl.BlockSpec((depth, 1), lambda e, w: (0, 0))],
            out_specs=(spec_out, spec_out),
        ),
        compiler_params=params(),
        cost_estimate=cost(3e9, 7e6),
        name="pack",
    )(where, gate, up, gain)


def unpack_kernel(where_ref, *refs):
    own, a, b = refs[0:2], refs[2:4], refs[4:6]
    gate_ref, up_ref = refs[6:8]
    z, tp = where_ref[0], where_ref[1]
    sources, _, half, lanes = own[0].shape
    left = lax.broadcasted_iota(jnp.int32, (half, lanes), 1) < lanes // 2
    for part in range(2):
        for side in range(2):
            for pair in range(sources // 2):
                two = []
                for src in (2 * pair, 2 * pair + 1):
                    c, ra, rb = (r[side][src, 0].astype(jnp.float32) for r in (own, a, b))
                    if part == 0:
                        two.append(jnp.where(z == 0, c, jnp.where(z == 1, rb, ra)))
                    else:
                        two.append(jnp.where(z == 3, c, jnp.where(z == 2, rb, ra)))
                one, other = two
                crossed = pltpu.roll(jnp.where(left, other, one), lanes // 2, 1)
                gate = jnp.where(left, one, crossed)
                up = jnp.where(left, crossed, other)
                start = part * sources * (lanes // 2) + pair * lanes
                row = tp if side == 0 else 1 - tp
                rows = pl.ds(pl.multiple_of(row * half, 16), half)
                gate_ref[0, rows, start : start + lanes] = gate.astype(jnp.bfloat16)
                up_ref[0, rows, start : start + lanes] = up.astype(jnp.bfloat16)


def unpack(where, pieces):
    sources, experts, half, lanes = pieces[0].shape
    width = 2 * sources * (lanes // 2)
    out = jax.ShapeDtypeStruct((experts, 2 * half, width), jnp.bfloat16)
    spec_in = pl.BlockSpec((sources, 1, half, lanes), lambda e, w: (0, e, 0, 0))
    spec_out = pl.BlockSpec((1, 2 * half, width), lambda e, w: (e, 0, 0))
    return pl.pallas_call(
        unpack_kernel,
        out_shape=(out, out),
        grid_spec=pltpu.PrefetchScalarGridSpec(
            num_scalar_prefetch=1,
            grid=(experts,),
            in_specs=[spec_in] * 6,
            out_specs=(spec_out, spec_out),
        ),
        compiler_params=params(),
        cost_estimate=cost(5e9, 14e6),
        name="unpack",
    )(where, *pieces)


def join_kernel(where_ref, *refs):
    out_ref = refs[-1]
    gr, tp = where_ref[2], where_ref[1]
    width = refs[0].shape[-1]
    places = (gr * 2 + tp, (1 - gr) * 2 + tp, gr * 2 + 1 - tp, (1 - gr) * 2 + 1 - tp)
    for ref, place in zip(refs[:-1], places):
        out_ref[0, :, pl.ds(pl.multiple_of(place * width, width), width)] = ref[0]


def join(where, quarters):
    experts, depth, width = quarters[0].shape
    spec_in = pl.BlockSpec((1, depth, width), lambda e, w: (e, 0, 0))
    return pl.pallas_call(
        join_kernel,
        out_shape=jax.ShapeDtypeStruct((experts, depth, 4 * width), jnp.bfloat16),
        grid_spec=pltpu.PrefetchScalarGridSpec(
            num_scalar_prefetch=1,
            grid=(experts,),
            in_specs=[spec_in] * 4,
            out_specs=pl.BlockSpec((1, depth, 4 * width), lambda e, w: (e, 0, 0)),
        ),
        compiler_params=params(),
        cost_estimate=cost(2e9, 5.5e6),
        name="join",
    )(where, *quarters)


def hidden_kernel(order_ref, tokens_ref, mix_ref, gate_ref, up_ref, out_ref, normed, mix):
    chunk = pl.program_id(0)
    dests, _, rows, _ = tokens_ref.shape
    for place in range(dests):
        dest = order_ref[chunk * dests + place]
        values = tokens_ref[dest, 0].astype(jnp.float32)
        scale = lax.rsqrt(jnp.mean(values * values, axis=-1, keepdims=True) + 1e-06)
        at = slice(place * rows, (place + 1) * rows)
        normed[at, :] = (values * scale).astype(jnp.bfloat16)
        mix[at, :] = mix_ref[dest, 0]
    dims = (((1,), (1,)), ((), ()))
    gate = lax.dot_general(normed[...], gate_ref[...], dims, preferred_element_type=jnp.float32)
    up = lax.dot_general(normed[...], up_ref[...], dims, preferred_element_type=jnp.float32)
    hidden = gate / (1.0 + jnp.exp(-gate)) * up
    experts = mix_ref.shape[-1]
    per = out_ref.shape[-1] // experts
    unit = lax.broadcasted_iota(jnp.int32, hidden.shape, 1)
    factor = mix[:, experts - 1 : experts]
    for e in range(experts - 2, -1, -1):
        factor = jnp.where(unit < (e + 1) * per, mix[:, e : e + 1], factor)
    out_ref[0] = (hidden * factor).astype(jnp.bfloat16)


def hidden_units(order, tokens, mix, gate, up):
    dests, chunks, rows, width = tokens.shape
    experts = mix.shape[-1]
    units = gate.shape[0]
    whole = pl.BlockSpec((units, width), lambda c, o: (0, 0))
    return pl.pallas_call(
        hidden_kernel,
        out_shape=jax.ShapeDtypeStruct((chunks, dests * rows, units), jnp.bfloat16),
        grid_spec=pltpu.PrefetchScalarGridSpec(
            num_scalar_prefetch=1,
            grid=(chunks,),
            in_specs=[
                pl.BlockSpec((dests, 1, rows, width), lambda c, o: (0, c, 0, 0)),
                pl.BlockSpec((dests, 1, rows, experts), lambda c, o: (0, c, 0, 0)),
                whole,
                whole,
            ],
            out_specs=pl.BlockSpec((1, dests * rows, units), lambda c, o: (c, 0, 0)),
            scratch_shapes=[
                pltpu.VMEM((dests * rows, width), jnp.bfloat16),
                pltpu.VMEM((dests * rows, experts), jnp.float32),
            ],
        ),
        compiler_params=params(),
        cost_estimate=cost(4 * chunks * dests * rows * width * units, 20e6),
        name="hidden",
    )(order, tokens, mix, gate, up)


def down_kernel(hidden_ref, down_ref, send_ref, keep_ref):
    half = send_ref.shape[0]
    for ref, at in ((send_ref, slice(half, 2 * half)), (keep_ref, slice(0, half))):
        product = jnp.dot(hidden_ref[0, at], down_ref[...], preferred_element_type=jnp.float32)
        ref[...] = product.astype(jnp.bfloat16)


def down_product(hidden, down, chunk):
    _, rows, units = hidden.shape
    width = down.shape[1]
    out = jax.ShapeDtypeStruct((rows // 2, width), jnp.bfloat16)
    half = pl.BlockSpec((rows // 2, width), lambda i: (0, 0))
    return pl.pallas_call(
        down_kernel,
        out_shape=(out, out),
        grid=(1,),
        in_specs=[
            pl.BlockSpec((1, rows, units), lambda i: (chunk, 0, 0)),
            pl.BlockSpec((units, width), lambda i: (0, 0)),
        ],
        out_specs=(half, half),
        compiler_params=params(),
        cost_estimate=cost(2 * rows * units * width, 6e6),
        name="down",
    )(hidden, down)


def swap(array, axis, mask):
    peers = lax.axis_size(axis)
    return lax.ppermute(array, axis, [(i, i ^ mask) for i in range(peers)])


def added(*terms):
    total = terms[0].astype(jnp.float32)
    for term in terms[1:]:
        total = total + term.astype(jnp.float32)
    return total


def near_order(me, mask):
    return [me, me ^ (4 - mask), me ^ mask, me ^ 2]


def chunk_order(first, mask):
    z, y, x = (lax.axis_index(a) for a in FS)
    ys, xs, zs = near_order(y, mask), near_order(x, mask), [z, z ^ 1]
    places = []
    for outer in range(4):
        for inner in range(4):
            for zz in zs:
                yy, xx = (ys[outer], xs[inner]) if first == "y" else (ys[inner], xs[outer])
                places.append(zz * 16 + yy * 4 + xx)
    return places


def butterfly(send, keep, first, mask, rows):
    axes = ("fs_1", "fs_2") if first == "y" else ("fs_2", "fs_1")
    width = send.shape[-1]
    shape = (2, 4, 2, rows, width)
    other = 4 - mask
    came = swap(send, axes[0], mask).reshape(shape)
    keep = keep.reshape(shape)
    sent = added(keep[1], came[1]).astype(jnp.bfloat16)
    back = swap(sent, axes[0], other)
    total = lambda i: added(keep[0, i], came[0, i], back[i])
    sent = jnp.stack([total(2), total(3)]).astype(jnp.bfloat16)
    came3 = swap(sent, axes[1], mask)
    sent = added(total(1), came3[1]).astype(jnp.bfloat16)
    back4 = swap(sent, axes[1], other)
    return added(total(0), came3[0], back4)


def mixing(chosen, weights, experts):
    share = weights / jnp.sum(weights, axis=-1, keepdims=True)
    labels = jnp.arange(experts, dtype=jnp.int32)
    match = (chosen[:, :, None] == labels[None, None, :]).astype(jnp.float32)
    return jnp.sum(share[:, :, None] * match, axis=1)


def shards(tokens, gate_master, up_master, down_master, norm_gain, route, route_weight):
    gr, tp = lax.axis_index("gr"), lax.axis_index("tp")
    z = lax.axis_index(Z)
    where = jnp.stack([z, tp, gr]).astype(jnp.int32)
    experts, depth, _ = gate_master.shape
    peers = lax.axis_size(("fs_1", "fs_2"))
    other_core = lambda v: swap(v, "tp", 1)

    down_own = down_master.astype(jnp.bfloat16)
    down_far = swap(down_own, "gr", 1)

    own, send = pack(where, gate_master, up_master, norm_gain[:, None], peers // 2)
    came = other_core(send)
    blocks = jnp.where(
        tp == 0, jnp.concatenate([own, came], axis=0), jnp.concatenate([came, own], axis=0)
    )
    mine = lax.all_to_all(blocks, ("fs_1", "fs_2"), split_axis=0, concat_axis=0, tiled=True)
    near = lax.ppermute(mine, Z, [(0, 2), (1, 0), (2, 3), (3, 1)])
    mid = lax.ppermute(mine, Z, [(1, 2), (2, 1)])
    pieces = []
    for piece in (mine, near, mid):
        pieces += [piece, other_core(piece)]

    quarters = [down_own, down_far, other_core(down_own), other_core(down_far)]
    down_out = join(where, quarters)
    gate_t, up_t = unpack(where, pieces)

    dests = lax.axis_size(FS)
    rows_in = tokens[0]
    count, width = rows_in.shape
    chunks = len(CHUNKS)
    rows = count // dests // chunks
    combine = mixing(route[0], route_weight[0], experts)
    order = [place for first, mask in CHUNKS for place in chunk_order(first, mask)]
    order = jnp.stack(order).astype(jnp.int32)
    hidden = hidden_units(
        order,
        rows_in.reshape(dests, chunks, rows, width),
        combine.reshape(dests, chunks, rows, experts),
        gate_t.reshape(-1, width),
        up_t.reshape(-1, width),
    )
    flat_down = down_out.reshape(-1, width)
    halves = []
    for chunk, (first, mask) in enumerate(CHUNKS):
        to_send, to_keep = down_product(hidden, flat_down, chunk)
        halves.append(butterfly(to_send, to_keep, first, mask, rows))
    sent = jnp.stack([h[1] for h in halves]).astype(jnp.bfloat16)
    came = swap(sent, "fs_0", 1)
    mixed = jnp.stack([added(h[0], came[i]) for i, h in enumerate(halves)])
    mixed = mixed.astype(jnp.bfloat16).reshape(1, chunks * rows, width)
    return (jnp.swapaxes(gate_t, 1, 2), jnp.swapaxes(up_t, 1, 2), down_out, mixed)


def solution(mesh):
    split = Mesh(
        mesh.devices.reshape(mesh.shape["gr"], 2, 4, 4, mesh.shape["tp"]),
        ("gr", "fs_0", "fs_1", "fs_2", "tp"),
    )
    in_specs = (
        P(("gr", "tp"), None, None),
        P(None, FS, ("gr", "tp")),
        P(None, FS, ("gr", "tp")),
        P(None, FS, ("gr", "tp")),
        P(FS),
        P(("gr", "tp"), None, None),
        P(("gr", "tp"), None, None),
    )
    out_specs = (P(None, None, FS), P(None, None, FS), P(None, FS, None), P(("gr", "tp"), FS, None))
    return jax.shard_map(
        shards, mesh=split, in_specs=in_specs, out_specs=out_specs, check_vma=False
    )
```

```python
import jax
import jax.numpy as jnp
from jax import lax
from jax.experimental import pallas as pl
from jax.experimental.pallas import tpu as pltpu
from jax.sharding import Mesh
from jax.sharding import PartitionSpec as P

FS = ("fs_0", "fs_1", "fs_2")
PLANE = ("fs_1", "fs_2")
Z = ("gr", "fs_0")
UNITS = 256
MIB = 1024 * 1024


COLORS = (("y", 1), ("x", 1), ("y", 3), ("x", 3))
WAVES = 2


def call(kernel, name, grid, ins, outs, out_shape, args, flops, nbytes, scratch=(), vmem=32):
    return pl.pallas_call(
        kernel,
        out_shape=out_shape,
        grid_spec=pltpu.PrefetchScalarGridSpec(
            num_scalar_prefetch=1,
            grid=grid,
            in_specs=ins,
            out_specs=outs,
            scratch_shapes=list(scratch),
        ),
        compiler_params=pltpu.CompilerParams(vmem_limit_bytes=vmem * MIB),
        cost_estimate=pl.CostEstimate(
            flops=int(flops), bytes_accessed=int(nbytes), transcendentals=0
        ),
        name=name,
    )(*args)


def whole(shape):
    return pl.BlockSpec(shape, lambda *_: (0,) * len(shape))


def shaped(*shape, dtype=jnp.bfloat16):
    return jax.ShapeDtypeStruct(shape, dtype)


def pack_kernel(where_ref, gate_ref, up_ref, gain_ref, own_ref, send_ref):
    rows = jnp.concatenate([gate_ref[0], up_ref[0]], axis=0)
    gain = jnp.concatenate([gain_ref[...], gain_ref[...]], axis=1)
    cols = (rows.T * gain).astype(jnp.bfloat16)
    dests, half, lanes = own_ref.shape
    cols = cols.reshape(dests, 2, half, lanes)
    low, high = cols[:, 0], cols[:, 1]
    first = where_ref[1] == 0
    own_ref[...] = jnp.where(first, low, high)
    send_ref[...] = jnp.where(first, high, low)


def pack(where, gate, up, gain, expert, dests):
    _, depth, width = gate.shape
    shape = (dests, width // dests // 2, 2 * depth)
    block = pl.BlockSpec((1, depth, width), lambda i, w: (expert, 0, 0))
    return call(
        pack_kernel, "pack", (1,), [block, block, whole((1, depth))], [whole(shape)] * 2,
        [shaped(*shape)] * 2, (where, gate, up, gain), 1e9, 2e6,
    )


def unpack_kernel(where_ref, own_ref, down_ref, up_ref, far_ref, out_ref):
    z = where_ref[0]
    sources, half, lanes = own_ref.shape
    left = lax.broadcasted_iota(jnp.int32, (half, lanes), 1) < lanes // 2
    pick = ((own_ref, down_ref, far_ref, up_ref), (down_ref, far_ref, up_ref, own_ref))
    for plane in range(4):

        @pl.when(z == plane)
        def _():
            for part in range(2):
                ref = pick[part][plane]
                for pair in range(sources // 2):
                    one = ref[2 * pair].astype(jnp.float32)
                    other = ref[2 * pair + 1].astype(jnp.float32)
                    crossed = pltpu.roll(jnp.where(left, other, one), lanes // 2, 1)
                    start = part * sources * (lanes // 2) + pair * lanes
                    at = slice(start, start + lanes)
                    out_ref[0, :, at] = jnp.where(left, one, crossed).astype(jnp.bfloat16)
                    out_ref[1, :, at] = jnp.where(left, crossed, other).astype(jnp.bfloat16)


def unpack(where, pieces):
    sources, half, lanes = pieces[0].shape
    shape = (2, half, sources * lanes)
    return call(
        unpack_kernel, "unpack", (1,), [whole(pieces[0].shape)] * 4, whole(shape),
        shaped(*shape), (where, *pieces), 1e9, 3e6,
    )


def assemble_kernel(where_ref, *refs):
    gate_ref, up_ref = refs[-2:]
    tp = where_ref[1]
    half = refs[0].shape[1]
    for index, ref in enumerate(refs[:-2]):
        side = tp if index % 2 == 0 else 1 - tp
        rows = pl.ds(pl.multiple_of(side * half, 16), half)
        gate_ref[index // 2, rows, :] = ref[0]
        up_ref[index // 2, rows, :] = ref[1]


def assemble(where, sides):
    _, half, width = sides[0].shape
    shape = (len(sides) // 2, 2 * half, width)
    return call(
        assemble_kernel, "assemble", (1,), [whole(sides[0].shape)] * len(sides),
        [whole(shape)] * 2, [shaped(*shape)] * 2, (where, *sides), 4e9, 11e6,
    )


def join_kernel(where_ref, *refs):
    out_ref, padded_ref = refs[-2:]
    tp, gr = where_ref[1], where_ref[2]
    depth, width = refs[0].shape[1:]
    places = (gr * 2 + tp, (1 - gr) * 2 + tp, gr * 2 + 1 - tp, (1 - gr) * 2 + 1 - tp)
    for ref, place in zip(refs[:-2], places):
        at = pl.ds(pl.multiple_of(place * width, width), width)
        out_ref[0, :, at] = ref[0]
        padded_ref[0, :depth, at] = ref[0]
    rest = padded_ref.shape[1] - depth
    padded_ref[0, depth:, :] = jnp.zeros((rest, padded_ref.shape[2]), jnp.bfloat16)


def join(where, quarters):
    experts, depth, width = quarters[0].shape
    at = lambda e, w: (e, 0, 0)
    return call(
        join_kernel, "join", (experts,), [pl.BlockSpec((1, depth, width), at)] * 4,
        [pl.BlockSpec((1, depth, 4 * width), at), pl.BlockSpec((1, UNITS, 4 * width), at)],
        [shaped(experts, depth, 4 * width), shaped(experts, UNITS, 4 * width)],
        (where, *quarters), 2e9, 8e6,
    )


def near(index, mask):
    return (0, 4 - mask, mask, 2)[index]


def norm_kernel(where_ref, tokens_ref, mix_ref, out_ref, mix_out_ref):
    color = pl.program_id(0) % len(COLORS)
    z, y, x = where_ref[0] % 2, where_ref[3], where_ref[4]
    rows = tokens_ref.shape[2]
    along = color % 2 == 0
    for place in range(tokens_ref.shape[0]):
        outer, inner, zz = place // 8, place // 2 % 4, place % 2
        a = jnp.where(color < 2, near(outer, 1), near(outer, 3))
        b = jnp.where(color < 2, near(inner, 1), near(inner, 3))
        yy = y ^ jnp.where(along, a, b)
        xx = x ^ jnp.where(along, b, a)
        dest = (z ^ zz) * 16 + yy * 4 + xx
        values = tokens_ref[dest, 0].astype(jnp.float32)
        scale = lax.rsqrt(jnp.mean(values * values, axis=-1, keepdims=True) + 1e-06)
        at = slice(place * rows, (place + 1) * rows)
        out_ref[0, at, :] = (values * scale).astype(jnp.bfloat16)
        mix_out_ref[0, at, :] = mix_ref[dest, 0]


def norm(where, tokens, mix):
    dests, groups, rows, width = tokens.shape
    experts = mix.shape[-1]
    block = lambda last: pl.BlockSpec((dests, 1, rows, last), lambda g, w: (0, g, 0, 0))
    out = lambda last: pl.BlockSpec((1, dests * rows, last), lambda g, w: (g, 0, 0))
    return call(
        norm_kernel, "norm", (groups,), [block(width), block(experts)], [out(width), out(experts)],
        [shaped(groups, dests * rows, width), shaped(groups, dests * rows, experts, dtype=jnp.float32)],
        (where, tokens, mix), 6e9, 17e6,
    )


def fill(where_ref, own_ref, other_ref, gate, up):
    tp = where_ref[1]
    half = own_ref.shape[1]
    for ref, side in ((own_ref, tp), (other_ref, 1 - tp)):
        rows = pl.ds(pl.multiple_of(side * half, 16), half)
        gate[rows, :] = ref[0]
        up[rows, :] = ref[1]
    rest = jnp.zeros((gate.shape[0] - 2 * half, gate.shape[1]), jnp.bfloat16)
    gate[2 * half :, :] = rest
    up[2 * half :, :] = rest


def hidden_of(normed, mix, gate, up):
    dims = (((1,), (1,)), ((), ()))
    gate_act = lax.dot_general(normed, gate, dims, preferred_element_type=jnp.float32)
    up_act = lax.dot_general(normed, up, dims, preferred_element_type=jnp.float32)
    return (gate_act / (1.0 + jnp.exp(-gate_act)) * up_act * mix).astype(jnp.bfloat16)


def hidden_kernel(expert, where_ref, normed_ref, mix_ref, own_ref, other_ref, out_ref, gate, up):
    @pl.when(pl.program_id(0) == 0)
    def _():
        fill(where_ref, own_ref, other_ref, gate, up)

    mix = mix_ref[0, :, expert : expert + 1]
    out_ref[0] = hidden_of(normed_ref[0], mix, gate[...], up[...])


def hidden_units(where, normed, mix, own, other, expert):
    groups, rows, width = normed.shape
    at = lambda g, w: (g, 0, 0)
    side = whole(own.shape)
    weight = pltpu.VMEM((UNITS, width), jnp.bfloat16)
    return call(
        lambda *refs: hidden_kernel(expert, *refs), "hidden", (groups,),
        [pl.BlockSpec((1, rows, width), at), pl.BlockSpec((1, rows, mix.shape[-1]), at), side, side],
        pl.BlockSpec((1, rows, UNITS), at), shaped(groups, rows, UNITS),
        (where, normed, mix, own, other), 4 * groups * rows * width * UNITS, 12e6,
        scratch=(weight, weight),
    )


def last_kernel(where_ref, normed_ref, mix_ref, *refs):
    earlier, (own_ref, other_ref, down_ref) = refs[:2], refs[2:5]
    outs, (gate, up) = refs[5:-2], refs[-2:]
    step = pl.program_id(0)

    @pl.when(step == 0)
    def _():
        fill(where_ref, own_ref, other_ref, gate, up)

    experts = down_ref.shape[0]
    mix = mix_ref[0, :, experts - 1 : experts]
    hidden = hidden_of(normed_ref[0], mix, gate[...], up[...])
    hidden = jnp.concatenate([r[0] for r in earlier] + [hidden], axis=1)
    half = outs[0].shape[0]
    here = hidden.shape[0] // (2 * half)
    down = down_ref[...].reshape(experts * UNITS, down_ref.shape[2])
    for color in range(here):
        rows = hidden[color * 2 * half : (color + 1) * 2 * half]
        product = jnp.dot(rows, down, preferred_element_type=jnp.float32).astype(jnp.bfloat16)
        for turn in range(len(COLORS) // here):

            @pl.when(step == turn)
            def _():
                send_ref, keep_ref = outs[2 * (turn * here + color) :][:2]
                keep_ref[...] = product[:half]
                send_ref[...] = product[half:]


def last(where, normed, mix, earlier, own, other, down, wave):
    groups, rows, width = normed.shape
    steps = groups // WAVES
    half = rows * steps // len(COLORS) // 2
    at = lambda g, w: (wave * steps + g, 0, 0)
    side = whole(own.shape)
    weight = pltpu.VMEM((UNITS, width), jnp.bfloat16)
    return call(
        last_kernel, "last", (steps,),
        [pl.BlockSpec((1, rows, width), at), pl.BlockSpec((1, rows, mix.shape[-1]), at)]
        + [pl.BlockSpec((1, rows, UNITS), at)] * 2 + [side, side, whole(down.shape)],
        [whole((half, width))] * 8, [shaped(half, width)] * 8,
        (where, normed, mix, *earlier, own, other, down), 10 * steps * rows * width * UNITS, 14e6,
        scratch=(weight, weight), vmem=48,
    )


def swap(array, axis, mask):
    peers = lax.axis_size(axis)
    return lax.ppermute(array, axis, [(i, i ^ mask) for i in range(peers)])


def added(*terms):
    total = terms[0].astype(jnp.float32)
    for term in terms[1:]:
        total = total + term.astype(jnp.float32)
    return total


def butterfly(send, keep, first, mask):
    axes = PLANE if first == "y" else PLANE[::-1]
    width = send.shape[-1]
    shape = (2, 4, 2, send.shape[0] // 16, width)
    other = 4 - mask
    came = swap(send, axes[0], mask).reshape(shape)
    keep = keep.reshape(shape)
    sent = added(keep[1], came[1]).astype(jnp.bfloat16)
    back = swap(sent, axes[0], other)
    total = lambda at: added(keep[0, at], came[0, at], back[at])
    sent = total(slice(2, 4)).astype(jnp.bfloat16)
    came3 = swap(sent, axes[1], mask)
    sent = added(total(1), came3[1]).astype(jnp.bfloat16)
    back4 = swap(sent, axes[1], other)
    return added(total(0), came3[0], back4)


def mixing(chosen, weights, experts):
    share = weights / jnp.sum(weights, axis=-1, keepdims=True)
    labels = jnp.arange(experts, dtype=jnp.int32)
    match = (chosen[:, :, None] == labels[None, None, :]).astype(jnp.float32)
    return jnp.sum(share[:, :, None] * match, axis=1)


def shards(tokens, gate_master, up_master, down_master, norm_gain, route, route_weight):
    z, tp = lax.axis_index(Z), lax.axis_index("tp")
    where = [z, tp, lax.axis_index("gr"), lax.axis_index("fs_1"), lax.axis_index("fs_2")]
    where = jnp.stack(where).astype(jnp.int32)
    experts = gate_master.shape[0]
    peers = lax.axis_size(PLANE)
    other_core = lambda v: swap(v, "tp", 1)
    gain = norm_gain[None, :]

    blocks = []
    for e in range(experts):
        own, send = pack(where, gate_master, up_master, gain, e, peers // 2)
        came = other_core(send)
        pair = jnp.where(
            tp == 0, jnp.concatenate([own, came], axis=0), jnp.concatenate([came, own], axis=0)
        )
        blocks.append(pair)

    down_own = down_master.astype(jnp.bfloat16)
    down_far = swap(down_own, "gr", 1)

    dests = lax.axis_size(FS)
    count, width = tokens.shape[1:]
    groups = len(COLORS) * WAVES
    rows = count // dests // groups
    combine = mixing(route[0], route_weight[0], experts)
    normed, mix = norm(
        where,
        tokens.reshape(dests, groups, rows, width),
        combine.reshape(dests, groups, rows, experts),
    )
    normed = normed.reshape(groups // 2, -1, width)
    mix = mix.reshape(groups // 2, -1, experts)

    quarters = [down_own, down_far, other_core(down_own), other_core(down_far)]
    down_out, down_padded = join(where, quarters)

    sides, earlier = [], []
    for e in range(experts):
        mine = lax.all_to_all(blocks[e], PLANE, split_axis=0, concat_axis=0, tiled=True)
        below = lax.ppermute(mine, Z, [(1, 0), (2, 1), (0, 3)])
        above = lax.ppermute(mine, Z, [(1, 2), (2, 3), (3, 0)])
        passed = jnp.where(z == 3, below, above)
        far = lax.ppermute(passed, Z, [(3, 2), (0, 1)])
        own = unpack(where, (mine, below, above, far))
        sides += [own, other_core(own)]
        if e < experts - 1:
            earlier.append(hidden_units(where, normed, mix, sides[-2], sides[-1], e))

    pieces = []
    for wave in range(WAVES):
        outs = last(where, normed, mix, earlier, sides[-2], sides[-1], down_padded, wave)
        halves = [
            butterfly(outs[2 * i], outs[2 * i + 1], *color) for i, color in enumerate(COLORS)
        ]
        sent = jnp.stack([h[1] for h in halves]).astype(jnp.bfloat16)
        came = swap(sent, "fs_0", 1)
        pieces += [added(h[0], came[i]).astype(jnp.bfloat16) for i, h in enumerate(halves)]
    mixed = jnp.concatenate(pieces, axis=0)[None]
    gate_t, up_t = assemble(where, sides)
    return (jnp.swapaxes(gate_t, 1, 2), jnp.swapaxes(up_t, 1, 2), down_out, mixed)


def solution(mesh):
    split = Mesh(
        mesh.devices.reshape(mesh.shape["gr"], 2, 4, 4, mesh.shape["tp"]),
        ("gr", "fs_0", "fs_1", "fs_2", "tp"),
    )
    in_specs = (
        P(("gr", "tp"), None, None),
        P(None, FS, ("gr", "tp")),
        P(None, FS, ("gr", "tp")),
        P(None, FS, ("gr", "tp")),
        P(FS),
        P(("gr", "tp"), None, None),
        P(("gr", "tp"), None, None),
    )
    out_specs = (P(None, None, FS), P(None, None, FS), P(None, FS, None), P(("gr", "tp"), FS, None))
    return jax.shard_map(
        shards, mesh=split, in_specs=in_specs, out_specs=out_specs, check_vma=False
    )
```

```python
import jax
import jax.numpy as jnp
from jax import lax
from jax.experimental import pallas as pl
from jax.experimental.pallas import tpu as pltpu
from jax.sharding import Mesh
from jax.sharding import PartitionSpec as P

FS = ("fs_0", "fs_1", "fs_2")
PLANE = ("fs_1", "fs_2")
Z = ("gr", "fs_0")
UNITS = 256
MIB = 1024 * 1024


COLORS = (
    (((1, 1), (1, 3), (2, 1), (2, 3)), 512),
    (((2, 1), (2, 3), (1, 1), (1, 3)), 384),
    (((1, 3), (1, 1), (2, 3), (2, 1)), 384),
    (((2, 3), (2, 1), (1, 3), (1, 1)), 384),
    (((0, 1), (1, 1), (1, 3), (2, 3), (2, 1)), 384),
)
CALLS = ((0, 1), (2, 3, 4))


def call(kernel, grid, ins, outs, out_shape, args, flops, nbytes, scratch=(), vmem=60):
    return pl.pallas_call(
        kernel,
        out_shape=out_shape,
        grid_spec=pltpu.PrefetchScalarGridSpec(
            num_scalar_prefetch=1,
            grid=grid,
            in_specs=ins,
            out_specs=outs,
            scratch_shapes=list(scratch),
        ),
        compiler_params=pltpu.CompilerParams(vmem_limit_bytes=vmem * MIB),
        cost_estimate=pl.CostEstimate(
            flops=int(flops), bytes_accessed=int(nbytes), transcendentals=0
        ),
    )(*args)


def whole(shape):
    return pl.BlockSpec(shape, lambda *_: (0,) * len(shape))


def shaped(*shape, dtype=jnp.bfloat16):
    return jax.ShapeDtypeStruct(shape, dtype)


def pack_kernel(where_ref, gate_ref, up_ref, gain_ref, own_ref, send_ref):
    rows = jnp.concatenate([gate_ref[0], up_ref[0]], axis=0)
    gain = jnp.concatenate([gain_ref[...], gain_ref[...]], axis=1)
    cols = (rows.T * gain).astype(jnp.bfloat16)
    dests, _, half, lanes = own_ref.shape
    cols = cols.reshape(dests, 2, half, lanes)
    low, high = cols[:, 0], cols[:, 1]
    first = where_ref[1] == 0
    own_ref[:, 0] = jnp.where(first, low, high)
    send_ref[:, 0] = jnp.where(first, high, low)


def pack(where, gate, up, gain, dests):
    experts, depth, width = gate.shape
    half = width // dests // 2
    block = pl.BlockSpec((1, depth, width), lambda e, w: (e, 0, 0))
    out = pl.BlockSpec((dests, 1, half, 2 * depth), lambda e, w: (0, e, 0, 0))
    return call(
        pack_kernel, (experts,), [block, block, whole((1, depth))], [out] * 2,
        [shaped(dests, experts, half, 2 * depth)] * 2, (where, gate, up, gain), 3e9, 6e6,
    )


def unpack_kernel(where_ref, own_ref, down_ref, up_ref, far_ref, out_ref):
    z = where_ref[0]
    sources, half, lanes = own_ref.shape
    left = lax.broadcasted_iota(jnp.int32, (half, lanes), 1) < lanes // 2
    pick = ((own_ref, down_ref, far_ref, up_ref), (down_ref, far_ref, up_ref, own_ref))
    for plane in range(4):

        @pl.when(z == plane)
        def _():
            for part in range(2):
                ref = pick[part][plane]
                for pair in range(sources // 2):
                    one = ref[2 * pair].astype(jnp.float32)
                    other = ref[2 * pair + 1].astype(jnp.float32)
                    crossed = pltpu.roll(jnp.where(left, other, one), lanes // 2, 1)
                    start = part * sources * (lanes // 2) + pair * lanes
                    at = slice(start, start + lanes)
                    out_ref[0, :, at] = jnp.where(left, one, crossed).astype(jnp.bfloat16)
                    out_ref[1, :, at] = jnp.where(left, crossed, other).astype(jnp.bfloat16)


def unpack(where, pieces):
    sources, half, lanes = pieces[0].shape
    shape = (2, half, sources * lanes)
    return call(
        unpack_kernel, (1,), [whole(pieces[0].shape)] * 4, whole(shape),
        shaped(*shape), (where, *pieces), 1e9, 3e6,
    )


def assemble_kernel(where_ref, *refs):
    gate_ref, up_ref = refs[-2:]
    tp = where_ref[1]
    half = refs[0].shape[1]
    for index, ref in enumerate(refs[:-2]):
        side = tp if index % 2 == 0 else 1 - tp
        rows = pl.ds(pl.multiple_of(side * half, 16), half)
        gate_ref[index // 2, rows, :] = ref[0]
        up_ref[index // 2, rows, :] = ref[1]


def assemble(where, sides):
    _, half, width = sides[0].shape
    shape = (len(sides) // 2, 2 * half, width)
    return call(
        assemble_kernel, (1,), [whole(sides[0].shape)] * len(sides),
        [whole(shape)] * 2, [shaped(*shape)] * 2, (where, *sides), 4e9, 11e6,
    )


def join_kernel(where_ref, *refs):
    out_ref, padded_ref = refs[-2:]
    tp, gr = where_ref[1], where_ref[2]
    depth, width = refs[0].shape[1:]
    places = (gr * 2 + tp, (1 - gr) * 2 + tp, gr * 2 + 1 - tp, (1 - gr) * 2 + 1 - tp)
    for ref, place in zip(refs[:-2], places):
        at = pl.ds(pl.multiple_of(place * width, width), width)
        out_ref[0, :, at] = ref[0]
        padded_ref[0, :depth, at] = ref[0]
    rest = padded_ref.shape[1] - depth
    padded_ref[0, depth:, :] = jnp.zeros((rest, padded_ref.shape[2]), jnp.bfloat16)


def join(where, quarters):
    experts, depth, width = quarters[0].shape
    at = lambda e, w: (e, 0, 0)
    return call(
        join_kernel, (experts,), [pl.BlockSpec((1, depth, width), at)] * 4,
        [pl.BlockSpec((1, depth, 4 * width), at), pl.BlockSpec((1, UNITS, 4 * width), at)],
        [shaped(experts, depth, 4 * width), shaped(experts, UNITS, 4 * width)],
        (where, *quarters), 2e9, 8e6,
    )


def norm_kernel(where_ref, tokens_ref, mix_ref, out_ref, mix_out_ref):
    z, x = where_ref[0] % 2, where_ref[4]
    rows = tokens_ref.shape[3]
    for place in range(8):
        zz, xx = z ^ (place % 2), x ^ (place // 2)
        values = tokens_ref[zz, 0, xx].astype(jnp.float32)
        scale = lax.rsqrt(jnp.mean(values * values, axis=-1, keepdims=True) + 1e-06)
        at = slice(place * rows, (place + 1) * rows)
        out_ref[0, at, :] = (values * scale).astype(jnp.bfloat16)
        mix_out_ref[0, at, :] = mix_ref[zz, 0, xx]


def norm(where, tokens, mix):
    zs, ys, xs, rows, width = tokens.shape
    experts = mix.shape[-1]
    block = lambda last: pl.BlockSpec((zs, 1, xs, rows, last), lambda i, w: (0, w[3] ^ i, 0, 0, 0))
    out = lambda last: pl.BlockSpec((1, xs * zs * rows, last), lambda i, w: (i, 0, 0))
    return call(
        norm_kernel, (ys,), [block(width), block(experts)], [out(width), out(experts)],
        [
            shaped(ys, xs * zs * rows, width),
            shaped(ys, xs * zs * rows, experts, dtype=jnp.float32),
        ],
        (where, tokens, mix), 6e9, 17e6,
    )


def fill(where_ref, own_ref, other_ref, gate, up):
    tp = where_ref[1]
    half = own_ref.shape[1]
    for ref, side in ((own_ref, tp), (other_ref, 1 - tp)):
        rows = pl.ds(pl.multiple_of(side * half, 16), half)
        gate[rows, :] = ref[0]
        up[rows, :] = ref[1]
    rest = jnp.zeros((gate.shape[0] - 2 * half, gate.shape[1]), jnp.bfloat16)
    gate[2 * half :, :] = rest
    up[2 * half :, :] = rest


def hidden_of(normed, mix, gate, up):
    dims = (((1,), (1,)), ((), ()))
    gate_act = lax.dot_general(normed, gate, dims, preferred_element_type=jnp.float32)
    up_act = lax.dot_general(normed, up, dims, preferred_element_type=jnp.float32)
    return (gate_act / (1.0 + jnp.exp(-gate_act)) * up_act * mix).astype(jnp.bfloat16)


def hidden_kernel(expert, where_ref, normed_ref, mix_ref, own_ref, other_ref, out_ref, gate, up):
    @pl.when(pl.program_id(0) == 0)
    def _():
        fill(where_ref, own_ref, other_ref, gate, up)

    mix = mix_ref[0, :, expert : expert + 1]
    out_ref[0] = hidden_of(normed_ref[0], mix, gate[...], up[...])


def hidden_units(where, normed, mix, own, other, expert):
    groups, rows, width = normed.shape
    at = lambda g, w: (g, 0, 0)
    side = whole(own.shape)
    weight = pltpu.VMEM((UNITS, width), jnp.bfloat16)
    return call(
        lambda *refs: hidden_kernel(expert, *refs), (groups,),
        [pl.BlockSpec((1, rows, width), at), pl.BlockSpec((1, rows, mix.shape[-1]), at), side, side],
        pl.BlockSpec((1, rows, UNITS), at), shaped(groups, rows, UNITS),
        (where, normed, mix, own, other), 4 * groups * rows * width * UNITS, 12e6,
        scratch=(weight, weight),
    )


def down_kernel(colors, starts, where_ref, *refs):
    hidden, down_ref, outs = refs[:3], refs[3], refs[4:]
    ys, block, _ = hidden[0].shape
    for yy in range(ys):
        rows = jnp.concatenate([h[yy] for h in hidden], axis=1)
        for index, ((exchanges, width), start) in enumerate(zip(colors, starts)):
            at = slice(start, start + width)
            product = jnp.dot(rows, down_ref[:, at], preferred_element_type=jnp.float32)
            product = product.astype(jnp.bfloat16)
            send_ref, keep_ref = outs[2 * index : 2 * index + 2]
            axis, mask = exchanges[0]
            place = {0: (keep_ref, 0), 4 - mask: (keep_ref, 1), mask: (send_ref, 0), 2: (send_ref, 1)}
            if axis == 1:
                ref, k = place[yy]
                ref[k * block : (k + 1) * block] = product
            elif axis == 2:
                part = block // 4
                for xx in range(4):
                    ref, k = place[xx]
                    to = (k * ys + yy) * part
                    ref[to : to + part] = product[xx * part : (xx + 1) * part]
            else:
                part = block // 8
                for xx in range(4):
                    to, at_x = (yy * 4 + xx) * part, 2 * xx * part
                    keep_ref[to : to + part] = product[at_x : at_x + part]
                    send_ref[to : to + part] = product[at_x + part : at_x + 2 * part]


def down_product(where, hidden, down, chosen):
    ys, block, units = hidden[0].shape
    half = ys * block // 2
    colors = [COLORS[c] for c in chosen]
    starts = [sum(width for _, width in COLORS[:c]) for c in chosen]
    outs = [(half, width) for _, width in colors for _ in range(2)]
    columns = sum(width for _, width in colors)
    return call(
        lambda *refs: down_kernel(colors, starts, *refs), (1,),
        [whole(hidden[0].shape)] * 3 + [whole(down.shape)],
        [whole(out) for out in outs], [shaped(*out) for out in outs],
        (where, *hidden, down), 2 * ys * block * 3 * units * columns, 10e6,
    )


def swap(array, axis, mask):
    peers = lax.axis_size(axis)
    return lax.ppermute(array, axis, [(i, i ^ mask) for i in range(peers)])


def added(terms):
    total = terms[0].astype(jnp.float32)
    for term in terms[1:]:
        total = total + term.astype(jnp.float32)
    return total


class Sums:
    def __init__(self, send, keep, exchanges):
        axis, mask = exchanges[0]
        self.axes = (axis, *(a for a in (1, 2, 0) if a != axis))
        sizes = [2 if a == 0 else 4 for a in self.axes]
        sizes[0] //= 2
        shape = (*sizes, -1, send.shape[-1])
        came = swap(send, FS[axis], mask).reshape(shape)
        self.offsets = [[0, 1, 2, 3] if a else [0, 1] for a in self.axes]
        self.offsets[0] = [0, 4 - mask] if axis else [0]
        places = [list(range(size)) for size in sizes]
        self.terms = [(keep.reshape(shape), places), (came, [list(p) for p in places])]

    def at(self, dim, index):
        parts = []
        for array, places in self.terms:
            for d, place in enumerate(places):
                if d == dim:
                    array = lax.slice_in_dim(array, place[index], place[index] + 1, axis=d)
                elif len(place) < array.shape[d]:
                    array = lax.slice_in_dim(array, place[0], place[0] + 1, axis=d)
            parts.append(array)
        return added(parts)

    def exchange(self, axis, mask):
        dim = self.axes.index(axis)
        have = self.offsets[dim]
        going, staying = ([mask], [0]) if len(have) == 2 else ([mask, 2], [0, 4 - mask])
        send = [self.at(dim, have.index(o)).astype(jnp.bfloat16) for o in going]
        came = swap(jnp.concatenate(send, axis=dim), FS[axis], mask)
        for _, places in self.terms:
            places[dim] = [places[dim][have.index(o)] for o in staying]
        self.terms.append((came, [list(range(size)) for size in came.shape[:3]]))
        self.offsets[dim] = staying

    def block(self, dim, index):
        total = self.at(dim, index)
        return total.reshape(total.shape[-2:])


def mixing(chosen, weights, experts):
    share = weights / jnp.sum(weights, axis=-1, keepdims=True)
    labels = jnp.arange(experts, dtype=jnp.int32)
    match = (chosen[:, :, None] == labels[None, None, :]).astype(jnp.float32)
    return jnp.sum(share[:, :, None] * match, axis=1)


def program(tokens, gate_master, up_master, down_master, norm_gain, route, route_weight):
    z, tp = lax.axis_index(Z), lax.axis_index("tp")
    where = [z, tp, lax.axis_index("gr"), lax.axis_index("fs_1"), lax.axis_index("fs_2")]
    where = jnp.stack(where).astype(jnp.int32)
    experts = gate_master.shape[0]
    peers = lax.axis_size(PLANE)
    other_core = lambda v: swap(v, "tp", 1)
    gain = norm_gain[None, :]

    own, send = pack(where, gate_master, up_master, gain, peers // 2)
    came = other_core(send)
    blocks = jnp.where(
        tp == 0, jnp.concatenate([own, came], axis=0), jnp.concatenate([came, own], axis=0)
    )
    mine = lax.all_to_all(blocks, PLANE, split_axis=0, concat_axis=0, tiled=True)

    down_own = down_master.astype(jnp.bfloat16)
    down_far = swap(down_own, "gr", 1)
    down_own_core, down_far_core = other_core(down_own), other_core(down_far)

    _, width = tokens.shape[1:]
    places = [lax.axis_size(a) for a in FS]
    combine = mixing(route[0], route_weight[0], experts)
    normed, mix = norm(
        where, tokens.reshape(*places, -1, width), combine.reshape(*places, -1, experts)
    )
    quarters = (down_own, down_far, down_own_core, down_far_core)
    mine, normed, quarters = lax.optimization_barrier((mine, normed, quarters))
    down_out, down_padded = join(where, quarters)

    sides, hidden = [], []
    for e in range(experts):
        piece = mine[:, e]
        below = lax.ppermute(piece, Z, [(1, 0), (2, 1), (0, 3)])
        above = lax.ppermute(piece, Z, [(1, 2), (2, 3), (3, 0)])
        passed = jnp.where(z == 3, below, above)
        far = lax.ppermute(passed, Z, [(3, 2), (0, 1)])
        own = unpack(where, (piece, below, above, far))
        sides += [own, other_core(own)]
        hidden.append(hidden_units(where, normed, mix, sides[-2], sides[-1], e))

    flat_down = down_padded.reshape(-1, width)
    sums = []
    for chosen in CALLS:
        outs = down_product(where, hidden, flat_down, chosen)
        for index, color in enumerate(chosen):
            sums.append(Sums(outs[2 * index], outs[2 * index + 1], COLORS[color][0]))
    for step in range(1, 5):
        for color, (exchanges, _) in zip(sums, COLORS):
            if step < len(exchanges):
                color.exchange(*exchanges[step])
    late = sums[:-1]
    sent = jnp.concatenate([c.block(2, 1).astype(jnp.bfloat16) for c in late], axis=1)
    came = swap(sent, "fs_0", 1)
    columns, start = [], 0
    for color, (_, span) in zip(late, COLORS):
        columns.append(added([color.block(2, 0), came[:, start : start + span]]))
        start += span
    columns.append(sums[-1].block(0, 0))
    mixed = jnp.concatenate([c.astype(jnp.bfloat16) for c in columns], axis=1)[None]
    gate_t, up_t = assemble(where, sides)
    return (jnp.swapaxes(gate_t, 1, 2), jnp.swapaxes(up_t, 1, 2), down_out, mixed)


def solution(mesh):
    split = Mesh(
        mesh.devices.reshape(mesh.shape["gr"], 2, 4, 4, mesh.shape["tp"]),
        ("gr", "fs_0", "fs_1", "fs_2", "tp"),
    )
    in_specs = (
        P(("gr", "tp"), None, None),
        P(None, FS, ("gr", "tp")),
        P(None, FS, ("gr", "tp")),
        P(None, FS, ("gr", "tp")),
        P(FS),
        P(("gr", "tp"), None, None),
        P(("gr", "tp"), None, None),
    )
    out_specs = (P(None, None, FS), P(None, None, FS), P(None, FS, None), P(("gr", "tp"), FS, None))
    return jax.shard_map(
        program, mesh=split, in_specs=in_specs, out_specs=out_specs, check_vma=False
    )
```

```python
import jax
import jax.numpy as jnp
from jax import lax
from jax.experimental import pallas as pl
from jax.experimental.pallas import tpu as pltpu
from jax.sharding import Mesh
from jax.sharding import PartitionSpec as P

FS = ("fs_0", "fs_1", "fs_2")
PLANE = ("fs_1", "fs_2")
Z = ("gr", "fs_0")
UNITS = 256
MIB = 1024 * 1024


COLORS = (
    ((1, 1), (1, 3), (2, 1), (2, 3)),
    ((2, 1), (2, 3), (1, 1), (1, 3)),
    ((1, 3), (1, 1), (2, 3), (2, 1)),
    ((2, 3), (2, 1), (1, 3), (1, 1)),
)


def call(kernel, grid, ins, outs, out_shape, args, flops, nbytes, scratch=(), vmem=60):
    return pl.pallas_call(
        kernel,
        out_shape=out_shape,
        grid_spec=pltpu.PrefetchScalarGridSpec(
            num_scalar_prefetch=1,
            grid=grid,
            in_specs=ins,
            out_specs=outs,
            scratch_shapes=list(scratch),
        ),
        compiler_params=pltpu.CompilerParams(vmem_limit_bytes=vmem * MIB),
        cost_estimate=pl.CostEstimate(
            flops=int(flops), bytes_accessed=int(nbytes), transcendentals=0
        ),
    )(*args)


def whole(shape):
    return pl.BlockSpec(shape, lambda *_: (0,) * len(shape))


def shaped(*shape, dtype=jnp.bfloat16):
    return jax.ShapeDtypeStruct(shape, dtype)


def pack_kernel(where_ref, gate_ref, up_ref, gain_ref, own_ref, send_ref):
    depth = gain_ref.shape[1]
    gain = jnp.broadcast_to(gain_ref[...], (128, depth)).T[:, :1]
    rows = jnp.concatenate([gate_ref[0] * gain, up_ref[0] * gain], axis=0)
    cols = rows.astype(jnp.bfloat16).T
    dests, _, half, lanes = own_ref.shape
    cols = cols.reshape(dests, 2, half, lanes)
    low, high = cols[:, 0], cols[:, 1]
    first = where_ref[1] == 0
    own_ref[:, 0] = jnp.where(first, low, high)
    send_ref[:, 0] = jnp.where(first, high, low)


def pack(where, gate, up, gain, dests):
    experts, depth, width = gate.shape
    half = width // dests // 2
    block = pl.BlockSpec((1, depth, width), lambda e, w: (e, 0, 0))
    out = pl.BlockSpec((dests, 1, half, 2 * depth), lambda e, w: (0, e, 0, 0))
    return call(
        pack_kernel, (experts,), [block, block, whole((1, depth))], [out] * 2,
        [shaped(dests, experts, half, 2 * depth)] * 2, (where, gate, up, gain), 3e9, 6e6,
    )


def unpack_kernel(where_ref, own_ref, down_ref, up_ref, far_ref, out_ref):
    z = where_ref[0]
    sources, half, lanes = own_ref.shape
    left = lax.broadcasted_iota(jnp.int32, (half, lanes), 1) < lanes // 2
    pick = ((own_ref, down_ref, far_ref, up_ref), (down_ref, far_ref, up_ref, own_ref))
    for plane in range(4):

        @pl.when(z == plane)
        def _():
            for part in range(2):
                ref = pick[part][plane]
                for pair in range(sources // 2):
                    one = ref[2 * pair].astype(jnp.float32)
                    other = ref[2 * pair + 1].astype(jnp.float32)
                    crossed = pltpu.roll(jnp.where(left, other, one), lanes // 2, 1)
                    start = part * sources * (lanes // 2) + pair * lanes
                    at = slice(start, start + lanes)
                    out_ref[0, :, at] = jnp.where(left, one, crossed).astype(jnp.bfloat16)
                    out_ref[1, :, at] = jnp.where(left, crossed, other).astype(jnp.bfloat16)


def unpack(where, pieces):
    sources, half, lanes = pieces[0].shape
    shape = (2, half, sources * lanes)
    return call(
        unpack_kernel, (1,), [whole(pieces[0].shape)] * 4, whole(shape),
        shaped(*shape), (where, *pieces), 1e9, 3e6, vmem=12,
    )


def assemble_kernel(where_ref, *refs):
    gate_ref, up_ref = refs[-2:]
    tp = where_ref[1]
    half = refs[0].shape[1]
    for index, ref in enumerate(refs[:-2]):
        side = tp if index % 2 == 0 else 1 - tp
        rows = pl.ds(pl.multiple_of(side * half, 16), half)
        gate_ref[index // 2, rows, :] = ref[0]
        up_ref[index // 2, rows, :] = ref[1]


def assemble(where, sides):
    _, half, width = sides[0].shape
    shape = (len(sides) // 2, 2 * half, width)
    return call(
        assemble_kernel, (1,), [whole(sides[0].shape)] * len(sides),
        [whole(shape)] * 2, [shaped(*shape)] * 2, (where, *sides), 4e9, 11e6, vmem=26,
    )


def join_kernel(where_ref, *refs):
    out_ref, padded_ref = refs[-2:]
    tp, gr = where_ref[1], where_ref[2]
    depth, width = refs[0].shape[1:]
    places = (gr * 2 + tp, (1 - gr) * 2 + tp, gr * 2 + 1 - tp, (1 - gr) * 2 + 1 - tp)
    for ref, place in zip(refs[:-2], places):
        at = pl.ds(pl.multiple_of(place * width, width), width)
        out_ref[0, :, at] = ref[0]
        padded_ref[0, :depth, at] = ref[0]
    rest = padded_ref.shape[1] - depth
    padded_ref[0, depth:, :] = jnp.zeros((rest, padded_ref.shape[2]), jnp.bfloat16)


def join(where, quarters):
    experts, depth, width = quarters[0].shape
    at = lambda e, w: (e, 0, 0)
    return call(
        join_kernel, (experts,), [pl.BlockSpec((1, depth, width), at)] * 4,
        [pl.BlockSpec((1, depth, 4 * width), at), pl.BlockSpec((1, UNITS, 4 * width), at)],
        [shaped(experts, depth, 4 * width), shaped(experts, UNITS, 4 * width)],
        (where, *quarters), 2e9, 8e6, vmem=16,
    )


def norm_kernel(where_ref, tokens_ref, mix_ref, out_ref, mix_out_ref):
    z, x = where_ref[0] % 2, where_ref[4]
    rows = tokens_ref.shape[3]
    for place in range(8):
        zz, xx = z ^ (place % 2), x ^ (place // 2)
        values = tokens_ref[zz, 0, xx].astype(jnp.float32)
        scale = lax.rsqrt(jnp.mean(values * values, axis=-1, keepdims=True) + 1e-06)
        at = slice(place * rows, (place + 1) * rows)
        out_ref[0, at, :] = (values * scale).astype(jnp.bfloat16)
        mix_out_ref[0, at, :] = mix_ref[zz, 0, xx]


def norm(where, tokens, mix):
    zs, ys, xs, rows, width = tokens.shape
    experts = mix.shape[-1]
    block = lambda last: pl.BlockSpec((zs, 1, xs, rows, last), lambda i, w: (0, w[3] ^ i, 0, 0, 0))
    out = lambda last: pl.BlockSpec((1, xs * zs * rows, last), lambda i, w: (i, 0, 0))
    return call(
        norm_kernel, (ys,), [block(width), block(experts)], [out(width), out(experts)],
        [
            shaped(ys, xs * zs * rows, width),
            shaped(ys, xs * zs * rows, experts, dtype=jnp.float32),
        ],
        (where, tokens, mix), 6e9, 17e6,
    )


def fill(where_ref, own_ref, other_ref, gate, up):
    tp = where_ref[1]
    half = own_ref.shape[1]
    for ref, side in ((own_ref, tp), (other_ref, 1 - tp)):
        rows = pl.ds(pl.multiple_of(side * half, 16), half)
        gate[rows, :] = ref[0]
        up[rows, :] = ref[1]
    rest = jnp.zeros((gate.shape[0] - 2 * half, gate.shape[1]), jnp.bfloat16)
    gate[2 * half :, :] = rest
    up[2 * half :, :] = rest


def hidden_of(normed, mix, gate, up):
    dims = (((1,), (1,)), ((), ()))
    gate_act = lax.dot_general(normed, gate, dims, preferred_element_type=jnp.float32)
    up_act = lax.dot_general(normed, up, dims, preferred_element_type=jnp.float32)
    return (gate_act / (1.0 + jnp.exp(-gate_act)) * up_act * mix).astype(jnp.bfloat16)


def hidden_kernel(expert, where_ref, normed_ref, mix_ref, own_ref, other_ref, out_ref, gate, up):
    @pl.when(pl.program_id(0) == 0)
    def _():
        fill(where_ref, own_ref, other_ref, gate, up)

    mix = mix_ref[0, :, expert : expert + 1]
    out_ref[0] = hidden_of(normed_ref[0], mix, gate[...], up[...])


def hidden_units(where, normed, mix, own, other, expert):
    groups, rows, width = normed.shape
    at = lambda g, w: (g, 0, 0)
    side = whole(own.shape)
    weight = pltpu.VMEM((UNITS, width), jnp.bfloat16)
    return call(
        lambda *refs: hidden_kernel(expert, *refs), (groups,),
        [pl.BlockSpec((1, rows, width), at), pl.BlockSpec((1, rows, mix.shape[-1]), at), side, side],
        pl.BlockSpec((1, rows, UNITS), at), shaped(groups, rows, UNITS),
        (where, normed, mix, own, other), 4 * groups * rows * width * UNITS, 12e6,
        scratch=(weight, weight), vmem=48,
    )


def last_kernel(where_ref, normed_ref, mix_ref, *refs):
    earlier, (own_ref, other_ref, down_ref) = refs[:2], refs[2:5]
    outs, (gate, up) = refs[5:-2], refs[-2:]
    yy = pl.program_id(0)

    @pl.when(yy == 0)
    def _():
        fill(where_ref, own_ref, other_ref, gate, up)

    experts = len(earlier) + 1
    mix = mix_ref[0, :, experts - 1 : experts]
    hidden = hidden_of(normed_ref[0], mix, gate[...], up[...])
    rows = jnp.concatenate([r[0] for r in earlier] + [hidden], axis=1)
    block = rows.shape[0]
    ys = pl.num_programs(0)
    width = outs[0].shape[1]
    for color, exchanges in enumerate(COLORS):
        at = slice(color * width, (color + 1) * width)
        product = jnp.dot(rows, down_ref[:, at], preferred_element_type=jnp.float32)
        product = product.astype(jnp.bfloat16)
        send_ref, keep_ref = outs[2 * color : 2 * color + 2]
        axis, mask = exchanges[0]
        if axis == 1:
            kept = (yy == 0) | (yy == 4 - mask)
            later = jnp.where((yy == 4 - mask) | (yy == 2), block, 0)
            to = pl.ds(pl.multiple_of(later, block), block)

            @pl.when(kept)
            def _():
                keep_ref[to, :] = product

            @pl.when(jnp.logical_not(kept))
            def _():
                send_ref[to, :] = product

        else:
            part = block // 4
            for xx, ref, k in ((0, keep_ref, 0), (4 - mask, keep_ref, 1), (mask, send_ref, 0), (2, send_ref, 1)):
                to = pl.ds(pl.multiple_of((k * ys + yy) * part, part), part)
                ref[to, :] = product[xx * part : (xx + 1) * part]


def last(where, normed, mix, earlier, own, other, down):
    ys, rows, width = normed.shape
    half = (ys * rows // 2, width // len(COLORS))
    at = lambda i, w: (i, 0, 0)
    side = whole(own.shape)
    weight = pltpu.VMEM((UNITS, width), jnp.bfloat16)
    return call(
        last_kernel, (ys,),
        [pl.BlockSpec((1, rows, width), at), pl.BlockSpec((1, rows, mix.shape[-1]), at)]
        + [pl.BlockSpec((1, rows, UNITS), at)] * 2 + [side, side, whole(down.shape)],
        [whole(half)] * (2 * len(COLORS)), [shaped(*half)] * (2 * len(COLORS)),
        (where, normed, mix, *earlier, own, other, down), 10 * ys * rows * width * UNITS, 25e6,
        scratch=(weight, weight), vmem=48,
    )


def swap(array, axis, mask):
    peers = lax.axis_size(axis)
    return lax.ppermute(array, axis, [(i, i ^ mask) for i in range(peers)])


def added(terms):
    total = terms[0].astype(jnp.float32)
    for term in terms[1:]:
        total = total + term.astype(jnp.float32)
    return total


class Sums:
    def __init__(self, send, keep, exchanges):
        axis, mask = exchanges[0]
        self.axes = (axis, *(a for a in (1, 2, 0) if a != axis))
        sizes = [2 if a == 0 else 4 for a in self.axes]
        sizes[0] //= 2
        shape = (*sizes, -1, send.shape[-1])
        came = swap(send, FS[axis], mask).reshape(shape)
        self.offsets = [[0, 1, 2, 3] if a else [0, 1] for a in self.axes]
        self.offsets[0] = [0, 4 - mask] if axis else [0]
        places = [list(range(size)) for size in sizes]
        self.terms = [(keep.reshape(shape), places), (came, [list(p) for p in places])]

    def at(self, dim, index):
        parts = []
        for array, places in self.terms:
            for d, place in enumerate(places):
                if d == dim:
                    array = lax.slice_in_dim(array, place[index], place[index] + 1, axis=d)
                elif len(place) < array.shape[d]:
                    array = lax.slice_in_dim(array, place[0], place[0] + 1, axis=d)
            parts.append(array)
        return added(parts)

    def exchange(self, axis, mask):
        dim = self.axes.index(axis)
        have = self.offsets[dim]
        going, staying = ([mask], [0]) if len(have) == 2 else ([mask, 2], [0, 4 - mask])
        send = [self.at(dim, have.index(o)).astype(jnp.bfloat16) for o in going]
        came = swap(jnp.concatenate(send, axis=dim), FS[axis], mask)
        for _, places in self.terms:
            places[dim] = [places[dim][have.index(o)] for o in staying]
        self.terms.append((came, [list(range(size)) for size in came.shape[:3]]))
        self.offsets[dim] = staying

    def block(self, dim, index):
        total = self.at(dim, index)
        return total.reshape(total.shape[-2:])


def mixing(chosen, weights, experts):
    share = weights / jnp.sum(weights, axis=-1, keepdims=True)
    labels = jnp.arange(experts, dtype=jnp.int32)
    match = (chosen[:, :, None] == labels[None, None, :]).astype(jnp.float32)
    return jnp.sum(share[:, :, None] * match, axis=1)


def program(tokens, gate_master, up_master, down_master, norm_gain, route, route_weight):
    z, tp = lax.axis_index(Z), lax.axis_index("tp")
    where = [z, tp, lax.axis_index("gr"), lax.axis_index("fs_1"), lax.axis_index("fs_2")]
    where = jnp.stack(where).astype(jnp.int32)
    experts = gate_master.shape[0]
    peers = lax.axis_size(PLANE)
    other_core = lambda v: swap(v, "tp", 1)
    gain = norm_gain[None, :]

    own, send = pack(where, gate_master, up_master, gain, peers // 2)
    came = other_core(send)
    blocks = jnp.where(
        tp == 0, jnp.concatenate([own, came], axis=0), jnp.concatenate([came, own], axis=0)
    )
    mine = lax.all_to_all(blocks, PLANE, split_axis=0, concat_axis=0, tiled=True)

    down_own = down_master.astype(jnp.bfloat16)
    down_far = swap(down_own, "gr", 1)
    down_own_core, down_far_core = other_core(down_own), other_core(down_far)

    _, width = tokens.shape[1:]
    places = [lax.axis_size(a) for a in FS]
    combine = mixing(route[0], route_weight[0], experts)
    normed, mix = norm(
        where, tokens.reshape(*places, -1, width), combine.reshape(*places, -1, experts)
    )
    quarters = (down_own, down_far, down_own_core, down_far_core)
    down_out, down_padded = join(where, quarters)
    mine, normed = lax.optimization_barrier((mine, normed))

    sides, hidden = [], []
    for e in range(experts):
        piece = mine[:, e]
        below = lax.ppermute(piece, Z, [(1, 0), (2, 1), (0, 3)])
        above = lax.ppermute(piece, Z, [(1, 2), (2, 3), (3, 0)])
        passed = jnp.where(z == 3, below, above)
        far = lax.ppermute(passed, Z, [(3, 2), (0, 1)])
        own = unpack(where, (piece, below, above, far))
        sides += [own, other_core(own)]
        if e < experts - 1:
            hidden.append(hidden_units(where, normed, mix, sides[-2], sides[-1], e))

    flat_down = down_padded.reshape(-1, width)
    outs = last(where, normed, mix, hidden, sides[-2], sides[-1], flat_down)
    sums = []
    for color, exchanges in enumerate(COLORS):
        sums.append(Sums(outs[2 * color], outs[2 * color + 1], exchanges))
    for step in range(1, 4):
        for color, exchanges in zip(sums, COLORS):
            color.exchange(*exchanges[step])
    sent = jnp.concatenate([c.block(2, 1).astype(jnp.bfloat16) for c in sums], axis=1)
    came = swap(sent, "fs_0", 1)
    mine = jnp.concatenate([c.block(2, 0) for c in sums], axis=1)
    mixed = added([mine, came]).astype(jnp.bfloat16)[None]
    gate_t, up_t = assemble(where, sides)
    return (jnp.swapaxes(gate_t, 1, 2), jnp.swapaxes(up_t, 1, 2), down_out, mixed)


def solution(mesh):
    split = Mesh(
        mesh.devices.reshape(mesh.shape["gr"], 2, 4, 4, mesh.shape["tp"]),
        ("gr", "fs_0", "fs_1", "fs_2", "tp"),
    )
    in_specs = (
        P(("gr", "tp"), None, None),
        P(None, FS, ("gr", "tp")),
        P(None, FS, ("gr", "tp")),
        P(None, FS, ("gr", "tp")),
        P(FS),
        P(("gr", "tp"), None, None),
        P(("gr", "tp"), None, None),
    )
    out_specs = (P(None, None, FS), P(None, None, FS), P(None, FS, None), P(("gr", "tp"), FS, None))
    return jax.shard_map(
        program, mesh=split, in_specs=in_specs, out_specs=out_specs, check_vma=False
    )
```

```python
import jax
import jax.numpy as jnp
from jax import lax
from jax.experimental import pallas as pl
from jax.experimental.pallas import tpu as pltpu
from jax.sharding import Mesh
from jax.sharding import PartitionSpec as P

FS = ("fs_0", "fs_1", "fs_2")
PLANE = ("fs_1", "fs_2")
Z = ("gr", "fs_0")
UNITS = 256
MIB = 1024 * 1024
LAST_VMEM = 40


COLORS = (
    ((1, 1), (1, 3), (2, 1), (2, 3)),
    ((2, 1), (2, 3), (1, 1), (1, 3)),
    ((1, 3), (1, 1), (2, 3), (2, 1)),
    ((2, 3), (2, 1), (1, 3), (1, 1)),
)


def call(kernel, grid, ins, outs, out_shape, args, flops, nbytes, scratch=(), vmem=60):
    return pl.pallas_call(
        kernel,
        out_shape=out_shape,
        grid_spec=pltpu.PrefetchScalarGridSpec(
            num_scalar_prefetch=1,
            grid=grid,
            in_specs=ins,
            out_specs=outs,
            scratch_shapes=list(scratch),
        ),
        compiler_params=pltpu.CompilerParams(vmem_limit_bytes=vmem * MIB),
        cost_estimate=pl.CostEstimate(
            flops=int(flops), bytes_accessed=int(nbytes), transcendentals=0
        ),
    )(*args)


def whole(shape):
    return pl.BlockSpec(shape, lambda *_: (0,) * len(shape))


def shaped(*shape, dtype=jnp.bfloat16):
    return jax.ShapeDtypeStruct(shape, dtype)


def pack_kernel(where_ref, gate_ref, up_ref, gain_ref, own_ref, send_ref):
    depth = gain_ref.shape[1]
    gain = jnp.broadcast_to(gain_ref[...], (128, depth)).T[:, :1]
    rows = jnp.concatenate([gate_ref[0] * gain, up_ref[0] * gain], axis=0)
    cols = rows.astype(jnp.bfloat16).T
    dests, _, half, lanes = own_ref.shape
    cols = cols.reshape(dests, 2, half, lanes)
    low, high = cols[:, 0], cols[:, 1]
    first = where_ref[1] == 0
    own_ref[:, 0] = jnp.where(first, low, high)
    send_ref[:, 0] = jnp.where(first, high, low)


def pack(where, gate, up, gain, dests):
    experts, depth, width = gate.shape
    half = width // dests // 2
    block = pl.BlockSpec((1, depth, width), lambda e, w: (e, 0, 0))
    out = pl.BlockSpec((dests, 1, half, 2 * depth), lambda e, w: (0, e, 0, 0))
    return call(
        pack_kernel, (experts,), [block, block, whole((1, depth))], [out] * 2,
        [shaped(dests, experts, half, 2 * depth)] * 2, (where, gate, up, gain), 3e9, 6e6,
    )


def unpack_kernel(where_ref, own_ref, down_ref, up_ref, far_ref, out_ref):
    z = where_ref[0]
    sources, half, lanes = own_ref.shape
    left = lax.broadcasted_iota(jnp.int32, (half, lanes), 1) < lanes // 2
    pick = ((own_ref, down_ref, far_ref, up_ref), (down_ref, far_ref, up_ref, own_ref))
    for plane in range(4):

        @pl.when(z == plane)
        def _():
            for part in range(2):
                ref = pick[part][plane]
                for pair in range(sources // 2):
                    one = ref[2 * pair].astype(jnp.float32)
                    other = ref[2 * pair + 1].astype(jnp.float32)
                    crossed = pltpu.roll(jnp.where(left, other, one), lanes // 2, 1)
                    start = part * sources * (lanes // 2) + pair * lanes
                    at = slice(start, start + lanes)
                    out_ref[0, :, at] = jnp.where(left, one, crossed).astype(jnp.bfloat16)
                    out_ref[1, :, at] = jnp.where(left, crossed, other).astype(jnp.bfloat16)


def unpack(where, pieces):
    sources, half, lanes = pieces[0].shape
    shape = (2, half, sources * lanes)
    return call(
        unpack_kernel, (1,), [whole(pieces[0].shape)] * 4, whole(shape),
        shaped(*shape), (where, *pieces), 1e9, 3e6, vmem=12,
    )


def assemble_kernel(where_ref, *refs):
    gate_ref, up_ref = refs[-2:]
    tp = where_ref[1]
    half = refs[0].shape[1]
    for index, ref in enumerate(refs[:-2]):
        side = tp if index % 2 == 0 else 1 - tp
        rows = pl.ds(pl.multiple_of(side * half, 16), half)
        gate_ref[index // 2, rows, :] = ref[0]
        up_ref[index // 2, rows, :] = ref[1]


def assemble(where, sides):
    _, half, width = sides[0].shape
    shape = (len(sides) // 2, 2 * half, width)
    return call(
        assemble_kernel, (1,), [whole(sides[0].shape)] * len(sides),
        [whole(shape)] * 2, [shaped(*shape)] * 2, (where, *sides), 4e9, 11e6, vmem=26,
    )


def join_kernel(where_ref, *refs):
    out_ref, padded_ref = refs[-2:]
    tp, gr = where_ref[1], where_ref[2]
    depth, width = refs[0].shape[1:]
    places = (gr * 2 + tp, (1 - gr) * 2 + tp, gr * 2 + 1 - tp, (1 - gr) * 2 + 1 - tp)
    for ref, place in zip(refs[:-2], places):
        at = pl.ds(pl.multiple_of(place * width, width), width)
        out_ref[0, :, at] = ref[0]
        padded_ref[0, :depth, at] = ref[0]
    rest = padded_ref.shape[1] - depth
    padded_ref[0, depth:, :] = jnp.zeros((rest, padded_ref.shape[2]), jnp.bfloat16)


def join(where, quarters):
    experts, depth, width = quarters[0].shape
    at = lambda e, w: (e, 0, 0)
    return call(
        join_kernel, (experts,), [pl.BlockSpec((1, depth, width), at)] * 4,
        [pl.BlockSpec((1, depth, 4 * width), at), pl.BlockSpec((1, UNITS, 4 * width), at)],
        [shaped(experts, depth, 4 * width), shaped(experts, UNITS, 4 * width)],
        (where, *quarters), 2e9, 8e6, vmem=16,
    )


def norm_kernel(where_ref, tokens_ref, mix_ref, out_ref, mix_out_ref):
    z, x = where_ref[0] % 2, where_ref[4]
    rows = tokens_ref.shape[3]
    for place in range(8):
        zz, xx = z ^ (place % 2), x ^ (place // 2)
        values = tokens_ref[zz, 0, xx].astype(jnp.float32)
        scale = lax.rsqrt(jnp.mean(values * values, axis=-1, keepdims=True) + 1e-06)
        at = slice(place * rows, (place + 1) * rows)
        out_ref[0, at, :] = (values * scale).astype(jnp.bfloat16)
        mix_out_ref[0, at, :] = mix_ref[zz, 0, xx]


def norm(where, tokens, mix):
    zs, ys, xs, rows, width = tokens.shape
    experts = mix.shape[-1]
    block = lambda last: pl.BlockSpec((zs, 1, xs, rows, last), lambda i, w: (0, w[3] ^ i, 0, 0, 0))
    out = lambda last: pl.BlockSpec((1, xs * zs * rows, last), lambda i, w: (i, 0, 0))
    return call(
        norm_kernel, (ys,), [block(width), block(experts)], [out(width), out(experts)],
        [
            shaped(ys, xs * zs * rows, width),
            shaped(ys, xs * zs * rows, experts, dtype=jnp.float32),
        ],
        (where, tokens, mix), 6e9, 17e6,
    )


def fill(where_ref, own_ref, other_ref, gate, up):
    tp = where_ref[1]
    half = own_ref.shape[1]
    for ref, side in ((own_ref, tp), (other_ref, 1 - tp)):
        rows = pl.ds(pl.multiple_of(side * half, 16), half)
        gate[rows, :] = ref[0]
        up[rows, :] = ref[1]
    rest = jnp.zeros((gate.shape[0] - 2 * half, gate.shape[1]), jnp.bfloat16)
    gate[2 * half :, :] = rest
    up[2 * half :, :] = rest


def hidden_of(normed, mix, gate, up):
    dims = (((1,), (1,)), ((), ()))
    gate_act = lax.dot_general(normed, gate, dims, preferred_element_type=jnp.float32)
    up_act = lax.dot_general(normed, up, dims, preferred_element_type=jnp.float32)
    return (gate_act / (1.0 + jnp.exp(-gate_act)) * up_act * mix).astype(jnp.bfloat16)


def hidden_kernel(expert, where_ref, normed_ref, mix_ref, own_ref, other_ref, out_ref, gate, up):
    @pl.when(pl.program_id(0) == 0)
    def _():
        fill(where_ref, own_ref, other_ref, gate, up)

    mix = mix_ref[0, :, expert : expert + 1]
    out_ref[0] = hidden_of(normed_ref[0], mix, gate[...], up[...])


def hidden_units(where, normed, mix, own, other, expert):
    groups, rows, width = normed.shape
    at = lambda g, w: (g, 0, 0)
    side = whole(own.shape)
    weight = pltpu.VMEM((UNITS, width), jnp.bfloat16)
    return call(
        lambda *refs: hidden_kernel(expert, *refs), (groups,),
        [pl.BlockSpec((1, rows, width), at), pl.BlockSpec((1, rows, mix.shape[-1]), at), side, side],
        pl.BlockSpec((1, rows, UNITS), at), shaped(groups, rows, UNITS),
        (where, normed, mix, own, other), 4 * groups * rows * width * UNITS, 12e6,
        scratch=(weight, weight), vmem=48,
    )


def last_kernel(where_ref, normed_ref, mix_ref, early_ref, *refs):
    sides, down_ref = (refs[0:2], refs[2:4]), refs[4]
    outs, weights = refs[5:-4], (refs[-4:-2], refs[-2:])
    yy = pl.program_id(0)

    @pl.when(yy == 0)
    def _():
        for side, weight in zip(sides, weights):
            fill(where_ref, *side, *weight)

    hidden = [early_ref[0]]
    for expert, (gate, up) in enumerate(weights, 1):
        mix = mix_ref[0, :, expert : expert + 1]
        hidden.append(hidden_of(normed_ref[0], mix, gate[...], up[...]))
    rows = jnp.concatenate(hidden, axis=1)
    block = rows.shape[0]
    ys = pl.num_programs(0)
    width = outs[0].shape[1]
    for color, exchanges in enumerate(COLORS):
        at = slice(color * width, (color + 1) * width)
        product = jnp.dot(rows, down_ref[:, at], preferred_element_type=jnp.float32)
        product = product.astype(jnp.bfloat16)
        send_ref, keep_ref = outs[2 * color : 2 * color + 2]
        axis, mask = exchanges[0]
        if axis == 1:
            kept = (yy == 0) | (yy == 4 - mask)
            later = jnp.where((yy == 4 - mask) | (yy == 2), block, 0)
            to = pl.ds(pl.multiple_of(later, block), block)

            @pl.when(kept)
            def _():
                keep_ref[to, :] = product

            @pl.when(jnp.logical_not(kept))
            def _():
                send_ref[to, :] = product

        else:
            part = block // 4
            for xx, ref, k in ((0, keep_ref, 0), (4 - mask, keep_ref, 1), (mask, send_ref, 0), (2, send_ref, 1)):
                to = pl.ds(pl.multiple_of((k * ys + yy) * part, part), part)
                ref[to, :] = product[xx * part : (xx + 1) * part]


def last(where, normed, mix, early, sides, down):
    ys, rows, width = normed.shape
    half = (ys * rows // 2, width // len(COLORS))
    at = lambda i, w: (i, 0, 0)
    side = whole(sides[0].shape)
    weight = pltpu.VMEM((UNITS, width), jnp.bfloat16)
    return call(
        last_kernel, (ys,),
        [pl.BlockSpec((1, rows, width), at), pl.BlockSpec((1, rows, mix.shape[-1]), at)]
        + [pl.BlockSpec((1, rows, UNITS), at)] + [side] * 4 + [whole(down.shape)],
        [whole(half)] * (2 * len(COLORS)), [shaped(*half)] * (2 * len(COLORS)),
        (where, normed, mix, early, *sides, down), 14 * ys * rows * width * UNITS, 25e6,
        scratch=(weight,) * 4, vmem=LAST_VMEM,
    )


def swap(array, axis, mask):
    peers = lax.axis_size(axis)
    return lax.ppermute(array, axis, [(i, i ^ mask) for i in range(peers)])


def added(terms):
    total = terms[0].astype(jnp.float32)
    for term in terms[1:]:
        total = total + term.astype(jnp.float32)
    return total


class Sums:
    def __init__(self, send, keep, exchanges):
        axis, mask = exchanges[0]
        self.axes = (axis, *(a for a in (1, 2, 0) if a != axis))
        sizes = [2 if a == 0 else 4 for a in self.axes]
        sizes[0] //= 2
        shape = (*sizes, -1, send.shape[-1])
        came = swap(send, FS[axis], mask).reshape(shape)
        self.offsets = [[0, 1, 2, 3] if a else [0, 1] for a in self.axes]
        self.offsets[0] = [0, 4 - mask] if axis else [0]
        places = [list(range(size)) for size in sizes]
        self.terms = [(keep.reshape(shape), places), (came, [list(p) for p in places])]

    def at(self, dim, index):
        parts = []
        for array, places in self.terms:
            for d, place in enumerate(places):
                if d == dim:
                    array = lax.slice_in_dim(array, place[index], place[index] + 1, axis=d)
                elif len(place) < array.shape[d]:
                    array = lax.slice_in_dim(array, place[0], place[0] + 1, axis=d)
            parts.append(array)
        return added(parts)

    def exchange(self, axis, mask):
        dim = self.axes.index(axis)
        have = self.offsets[dim]
        going, staying = ([mask], [0]) if len(have) == 2 else ([mask, 2], [0, 4 - mask])
        send = [self.at(dim, have.index(o)).astype(jnp.bfloat16) for o in going]
        came = swap(jnp.concatenate(send, axis=dim), FS[axis], mask)
        for _, places in self.terms:
            places[dim] = [places[dim][have.index(o)] for o in staying]
        self.terms.append((came, [list(range(size)) for size in came.shape[:3]]))
        self.offsets[dim] = staying

    def block(self, dim, index):
        total = self.at(dim, index)
        return total.reshape(total.shape[-2:])


def mixing(chosen, weights, experts):
    share = weights / jnp.sum(weights, axis=-1, keepdims=True)
    labels = jnp.arange(experts, dtype=jnp.int32)
    match = (chosen[:, :, None] == labels[None, None, :]).astype(jnp.float32)
    return jnp.sum(share[:, :, None] * match, axis=1)


def program(tokens, gate_master, up_master, down_master, norm_gain, route, route_weight):
    z, tp = lax.axis_index(Z), lax.axis_index("tp")
    where = [z, tp, lax.axis_index("gr"), lax.axis_index("fs_1"), lax.axis_index("fs_2")]
    where = jnp.stack(where).astype(jnp.int32)
    experts = gate_master.shape[0]
    peers = lax.axis_size(PLANE)
    other_core = lambda v: swap(v, "tp", 1)
    gain = norm_gain[None, :]

    own, send = pack(where, gate_master, up_master, gain, peers // 2)
    came = other_core(send)
    blocks = jnp.where(
        tp == 0, jnp.concatenate([own, came], axis=0), jnp.concatenate([came, own], axis=0)
    )
    mine = lax.all_to_all(blocks, PLANE, split_axis=0, concat_axis=0, tiled=True)

    down_own = down_master.astype(jnp.bfloat16)
    down_far = swap(down_own, "gr", 1)
    down_own_core, down_far_core = other_core(down_own), other_core(down_far)

    _, width = tokens.shape[1:]
    places = [lax.axis_size(a) for a in FS]
    combine = mixing(route[0], route_weight[0], experts)
    normed, mix = norm(
        where, tokens.reshape(*places, -1, width), combine.reshape(*places, -1, experts)
    )
    quarters = (down_own, down_far, down_own_core, down_far_core)
    down_out, down_padded = join(where, quarters)
    mine, normed = lax.optimization_barrier((mine, normed))

    sides = []
    for e in range(experts):
        piece = mine[:, e]
        below = lax.ppermute(piece, Z, [(1, 0), (2, 1), (0, 3)])
        above = lax.ppermute(piece, Z, [(1, 2), (2, 3), (3, 0)])
        passed = jnp.where(z == 3, below, above)
        far = lax.ppermute(passed, Z, [(3, 2), (0, 1)])
        own = unpack(where, (piece, below, above, far))
        sides += [own, other_core(own)]
    early = hidden_units(where, normed, mix, sides[0], sides[1], 0)
    outs = last(where, normed, mix, early, sides[2:], down_padded.reshape(-1, width))
    sums = []
    for color, exchanges in enumerate(COLORS):
        sums.append(Sums(outs[2 * color], outs[2 * color + 1], exchanges))
    for step in range(1, 4):
        for color, exchanges in zip(sums, COLORS):
            color.exchange(*exchanges[step])
    sent = jnp.concatenate([c.block(2, 1).astype(jnp.bfloat16) for c in sums], axis=1)
    came = swap(sent, "fs_0", 1)
    mine = jnp.concatenate([c.block(2, 0) for c in sums], axis=1)
    mixed = added([mine, came]).astype(jnp.bfloat16)[None]
    gate_t, up_t = assemble(where, sides)
    return (jnp.swapaxes(gate_t, 1, 2), jnp.swapaxes(up_t, 1, 2), down_out, mixed)


def solution(mesh):
    split = Mesh(
        mesh.devices.reshape(mesh.shape["gr"], 2, 4, 4, mesh.shape["tp"]),
        ("gr", "fs_0", "fs_1", "fs_2", "tp"),
    )
    in_specs = (
        P(("gr", "tp"), None, None),
        P(None, FS, ("gr", "tp")),
        P(None, FS, ("gr", "tp")),
        P(None, FS, ("gr", "tp")),
        P(FS),
        P(("gr", "tp"), None, None),
        P(("gr", "tp"), None, None),
    )
    out_specs = (P(None, None, FS), P(None, None, FS), P(None, FS, None), P(("gr", "tp"), FS, None))
    return jax.shard_map(
        program, mesh=split, in_specs=in_specs, out_specs=out_specs, check_vma=False
    )
```

```python
import jax
import jax.numpy as jnp
from jax import lax
from jax.experimental import pallas as pl
from jax.experimental.pallas import tpu as pltpu
from jax.sharding import Mesh
from jax.sharding import PartitionSpec as P

FS = ("fs_0", "fs_1", "fs_2")
PLANE = ("fs_1", "fs_2")
Z = ("gr", "fs_0")
UNITS = 256
MIB = 1024 * 1024
LAST_VMEM = 40


COLORS = (
    ((1, 1), (1, 3), (2, 1), (2, 3)),
    ((2, 1), (2, 3), (1, 1), (1, 3)),
    ((1, 3), (1, 1), (2, 3), (2, 1)),
    ((2, 3), (2, 1), (1, 3), (1, 1)),
)


def call(kernel, grid, ins, outs, out_shape, args, flops, nbytes, scratch=(), vmem=60):
    return pl.pallas_call(
        kernel,
        out_shape=out_shape,
        grid_spec=pltpu.PrefetchScalarGridSpec(
            num_scalar_prefetch=1,
            grid=grid,
            in_specs=ins,
            out_specs=outs,
            scratch_shapes=list(scratch),
        ),
        compiler_params=pltpu.CompilerParams(vmem_limit_bytes=vmem * MIB),
        cost_estimate=pl.CostEstimate(
            flops=int(flops), bytes_accessed=int(nbytes), transcendentals=0
        ),
    )(*args)


def whole(shape):
    return pl.BlockSpec(shape, lambda *_: (0,) * len(shape))


def shaped(*shape, dtype=jnp.bfloat16):
    return jax.ShapeDtypeStruct(shape, dtype)


def pack_kernel(where_ref, gate_ref, up_ref, gain_ref, *out_refs):
    depth = gain_ref.shape[1]
    gain = jnp.broadcast_to(gain_ref[...], (128, depth)).T[:, :1]
    rows = jnp.concatenate([gate_ref[0] * gain, up_ref[0] * gain], axis=0)
    cols = rows.astype(jnp.bfloat16).T
    dests, half, lanes = out_refs[-1].shape
    cols = cols.reshape(dests, 2, half, lanes)
    low, high = cols[:, 0], cols[:, 1]
    first = where_ref[1] == 0
    own, send = jnp.where(first, low, high), jnp.where(first, high, low)
    final = pl.program_id(0) == pl.num_programs(0) - 1

    @pl.when(jnp.logical_not(final))
    def _():
        out_refs[0][:, 0] = own
        out_refs[1][:, 0] = send

    @pl.when(final)
    def _():
        out_refs[2][...] = own
        out_refs[3][...] = send


def pack(where, gate, up, gain, dests):
    experts, depth, width = gate.shape
    half = width // dests // 2
    block = pl.BlockSpec((1, depth, width), lambda e, w: (e, 0, 0))
    one = (dests, half, 2 * depth)
    some = pl.BlockSpec((dests, 1, half, 2 * depth), lambda e, w: (0, jnp.minimum(e, experts - 2), 0, 0))
    return call(
        pack_kernel, (experts,), [block, block, whole((1, depth))],
        [some, some, whole(one), whole(one)],
        [shaped(dests, experts - 1, half, 2 * depth)] * 2 + [shaped(*one)] * 2,
        (where, gate, up, gain), 3e9, 6e6,
    )


def unpack_kernel(where_ref, *refs):
    out_ref = refs[-1]
    if len(refs) == 2:
        sources = refs[0].shape[0]
        choices = [[lambda s, part=part: refs[0][s, part] for part in range(2)]]
    else:
        own, below, above, far = refs[:-1]
        sources = own.shape[0]
        pick = ((own, below), (below, far), (far, above), (above, own))
        choices = [[lambda s, ref=ref: ref[s] for ref in two] for two in pick]
    half, lanes = refs[0].shape[-2:]
    left = lax.broadcasted_iota(jnp.int32, (half, lanes), 1) < lanes // 2

    def place(blocks):
        for part, block in enumerate(blocks):
            for pair in range(sources // 2):
                one = block(2 * pair).astype(jnp.float32)
                other = block(2 * pair + 1).astype(jnp.float32)
                crossed = pltpu.roll(jnp.where(left, other, one), lanes // 2, 1)
                start = part * sources * (lanes // 2) + pair * lanes
                at = slice(start, start + lanes)
                out_ref[0, :, at] = jnp.where(left, one, crossed).astype(jnp.bfloat16)
                out_ref[1, :, at] = jnp.where(left, crossed, other).astype(jnp.bfloat16)

    if len(choices) == 1:
        place(choices[0])
    else:
        for plane, blocks in enumerate(choices):
            pl.when(where_ref[0] == plane)(lambda blocks=blocks: place(blocks))


def unpack(where, pieces):
    sources = pieces[0].shape[0]
    half, lanes = pieces[0].shape[-2:]
    shape = (2, half, sources * lanes)
    return call(
        unpack_kernel, (1,), [whole(piece.shape) for piece in pieces], whole(shape),
        shaped(*shape), (where, *pieces), 1e9, 3e6, vmem=12,
    )


def assemble_kernel(where_ref, *refs):
    gate_ref, up_ref = refs[-2:]
    tp = where_ref[1]
    half = refs[0].shape[1]
    for index, ref in enumerate(refs[:-2]):
        side = tp if index % 2 == 0 else 1 - tp
        rows = pl.ds(pl.multiple_of(side * half, 16), half)
        gate_ref[index // 2, rows, :] = ref[0]
        up_ref[index // 2, rows, :] = ref[1]


def assemble(where, sides):
    _, half, width = sides[0].shape
    shape = (len(sides) // 2, 2 * half, width)
    return call(
        assemble_kernel, (1,), [whole(sides[0].shape)] * len(sides),
        [whole(shape)] * 2, [shaped(*shape)] * 2, (where, *sides), 4e9, 11e6, vmem=26,
    )


def join_kernel(where_ref, *refs):
    out_ref, padded_ref = refs[-2:]
    tp, gr = where_ref[1], where_ref[2]
    depth, width = refs[0].shape[1:]
    places = (gr * 2 + tp, (1 - gr) * 2 + tp, gr * 2 + 1 - tp, (1 - gr) * 2 + 1 - tp)
    for ref, place in zip(refs[:-2], places):
        at = pl.ds(pl.multiple_of(place * width, width), width)
        out_ref[0, :, at] = ref[0]
        padded_ref[0, :depth, at] = ref[0]
    rest = padded_ref.shape[1] - depth
    padded_ref[0, depth:, :] = jnp.zeros((rest, padded_ref.shape[2]), jnp.bfloat16)


def join(where, quarters):
    experts, depth, width = quarters[0].shape
    at = lambda e, w: (e, 0, 0)
    return call(
        join_kernel, (experts,), [pl.BlockSpec((1, depth, width), at)] * 4,
        [pl.BlockSpec((1, depth, 4 * width), at), pl.BlockSpec((1, UNITS, 4 * width), at)],
        [shaped(experts, depth, 4 * width), shaped(experts, UNITS, 4 * width)],
        (where, *quarters), 2e9, 8e6, vmem=16,
    )


def norm_kernel(where_ref, tokens_ref, mix_ref, out_ref, mix_out_ref):
    z, x = where_ref[0] % 2, where_ref[4]
    rows = tokens_ref.shape[3]
    for place in range(8):
        zz, xx = z ^ (place % 2), x ^ (place // 2)
        values = tokens_ref[zz, 0, xx].astype(jnp.float32)
        scale = lax.rsqrt(jnp.mean(values * values, axis=-1, keepdims=True) + 1e-06)
        at = slice(place * rows, (place + 1) * rows)
        out_ref[0, at, :] = (values * scale).astype(jnp.bfloat16)
        mix_out_ref[0, at, :] = mix_ref[zz, 0, xx]


def norm(where, tokens, mix):
    zs, ys, xs, rows, width = tokens.shape
    experts = mix.shape[-1]
    block = lambda last: pl.BlockSpec((zs, 1, xs, rows, last), lambda i, w: (0, w[3] ^ i, 0, 0, 0))
    out = lambda last: pl.BlockSpec((1, xs * zs * rows, last), lambda i, w: (i, 0, 0))
    return call(
        norm_kernel, (ys,), [block(width), block(experts)], [out(width), out(experts)],
        [
            shaped(ys, xs * zs * rows, width),
            shaped(ys, xs * zs * rows, experts, dtype=jnp.float32),
        ],
        (where, tokens, mix), 6e9, 17e6,
    )


def fill(where_ref, own_ref, other_ref, gate, up):
    tp = where_ref[1]
    half = own_ref.shape[1]
    for ref, side in ((own_ref, tp), (other_ref, 1 - tp)):
        rows = pl.ds(pl.multiple_of(side * half, 16), half)
        gate[rows, :] = ref[0]
        up[rows, :] = ref[1]
    rest = jnp.zeros((gate.shape[0] - 2 * half, gate.shape[1]), jnp.bfloat16)
    gate[2 * half :, :] = rest
    up[2 * half :, :] = rest


def hidden_of(normed, mix, gate, up):
    dims = (((1,), (1,)), ((), ()))
    gate_act = lax.dot_general(normed, gate, dims, preferred_element_type=jnp.float32)
    up_act = lax.dot_general(normed, up, dims, preferred_element_type=jnp.float32)
    return (gate_act / (1.0 + jnp.exp(-gate_act)) * up_act * mix).astype(jnp.bfloat16)


def last_kernel(experts, where_ref, normed_ref, mix_ref, *refs):
    sides = [refs[2 * e : 2 * e + 2] for e in range(experts)]
    down_ref, outs = refs[2 * experts], refs[2 * experts + 1 : -2 * experts]
    scratch = refs[-2 * experts :]
    weights = [scratch[2 * e : 2 * e + 2] for e in range(experts)]
    yy = pl.program_id(0)

    @pl.when(yy == 0)
    def _():
        for side, weight in zip(sides, weights):
            fill(where_ref, *side, *weight)

    hidden = []
    for expert, (gate, up) in enumerate(weights):
        mix = mix_ref[0, :, expert : expert + 1]
        hidden.append(hidden_of(normed_ref[0], mix, gate[...], up[...]))
    rows = jnp.concatenate(hidden, axis=1)
    block = rows.shape[0]
    ys = pl.num_programs(0)
    width = outs[0].shape[1]
    for color, exchanges in enumerate(COLORS):
        at = slice(color * width, (color + 1) * width)
        product = jnp.dot(rows, down_ref[:, at], preferred_element_type=jnp.float32)
        product = product.astype(jnp.bfloat16)
        send_ref, keep_ref = outs[2 * color : 2 * color + 2]
        axis, mask = exchanges[0]
        if axis == 1:
            kept = (yy == 0) | (yy == 4 - mask)
            later = jnp.where((yy == 4 - mask) | (yy == 2), block, 0)
            to = pl.ds(pl.multiple_of(later, block), block)

            @pl.when(kept)
            def _():
                keep_ref[to, :] = product

            @pl.when(jnp.logical_not(kept))
            def _():
                send_ref[to, :] = product

        else:
            part = block // 4
            for xx, ref, k in ((0, keep_ref, 0), (4 - mask, keep_ref, 1), (mask, send_ref, 0), (2, send_ref, 1)):
                to = pl.ds(pl.multiple_of((k * ys + yy) * part, part), part)
                ref[to, :] = product[xx * part : (xx + 1) * part]


def last(where, normed, mix, sides, down):
    ys, rows, width = normed.shape
    experts = len(sides) // 2
    half = (ys * rows // 2, width // len(COLORS))
    at = lambda i, w: (i, 0, 0)
    side = whole(sides[0].shape)
    weight = pltpu.VMEM((UNITS, width), jnp.bfloat16)
    return call(
        lambda *refs: last_kernel(experts, *refs), (ys,),
        [pl.BlockSpec((1, rows, width), at), pl.BlockSpec((1, rows, experts), at)]
        + [side] * (2 * experts) + [whole(down.shape)],
        [whole(half)] * (2 * len(COLORS)), [shaped(*half)] * (2 * len(COLORS)),
        (where, normed, mix, *sides, down), 6 * experts * ys * rows * width * UNITS, 25e6,
        scratch=(weight,) * (2 * experts), vmem=LAST_VMEM,
    )


def swap(array, axis, mask):
    peers = lax.axis_size(axis)
    return lax.ppermute(array, axis, [(i, i ^ mask) for i in range(peers)])


def added(terms):
    total = terms[0].astype(jnp.float32)
    for term in terms[1:]:
        total = total + term.astype(jnp.float32)
    return total


class Sums:
    def __init__(self, send, keep, exchanges):
        axis, mask = exchanges[0]
        self.axes = (axis, *(a for a in (1, 2, 0) if a != axis))
        sizes = [2 if a == 0 else 4 for a in self.axes]
        sizes[0] //= 2
        shape = (*sizes, -1, send.shape[-1])
        came = swap(send, FS[axis], mask).reshape(shape)
        self.offsets = [[0, 1, 2, 3] if a else [0, 1] for a in self.axes]
        self.offsets[0] = [0, 4 - mask] if axis else [0]
        places = [list(range(size)) for size in sizes]
        self.terms = [(keep.reshape(shape), places), (came, [list(p) for p in places])]

    def at(self, dim, index):
        parts = []
        for array, places in self.terms:
            for d, place in enumerate(places):
                if d == dim:
                    array = lax.slice_in_dim(array, place[index], place[index] + 1, axis=d)
                elif len(place) < array.shape[d]:
                    array = lax.slice_in_dim(array, place[0], place[0] + 1, axis=d)
            parts.append(array)
        return added(parts)

    def exchange(self, axis, mask):
        dim = self.axes.index(axis)
        have = self.offsets[dim]
        going, staying = ([mask], [0]) if len(have) == 2 else ([mask, 2], [0, 4 - mask])
        send = [self.at(dim, have.index(o)).astype(jnp.bfloat16) for o in going]
        came = swap(jnp.concatenate(send, axis=dim), FS[axis], mask)
        for _, places in self.terms:
            places[dim] = [places[dim][have.index(o)] for o in staying]
        self.terms.append((came, [list(range(size)) for size in came.shape[:3]]))
        self.offsets[dim] = staying

    def block(self, dim, index):
        total = self.at(dim, index)
        return total.reshape(total.shape[-2:])


def mixing(chosen, weights, experts):
    share = weights / jnp.sum(weights, axis=-1, keepdims=True)
    labels = jnp.arange(experts, dtype=jnp.int32)
    match = (chosen[:, :, None] == labels[None, None, :]).astype(jnp.float32)
    return jnp.sum(share[:, :, None] * match, axis=1)


def program(tokens, gate_master, up_master, down_master, norm_gain, route, route_weight):
    z, tp = lax.axis_index(Z), lax.axis_index("tp")
    where = [z, tp, lax.axis_index("gr"), lax.axis_index("fs_1"), lax.axis_index("fs_2")]
    where = jnp.stack(where).astype(jnp.int32)
    experts = gate_master.shape[0]
    peers = lax.axis_size(PLANE)
    other_core = lambda v: swap(v, "tp", 1)
    gain = norm_gain[None, :]

    own, send, own_last, send_last = pack(where, gate_master, up_master, gain, peers // 2)

    def whole_plane(own, send):
        came = other_core(send)
        orders = [jnp.concatenate(two, axis=0) for two in ((own, came), (came, own))]
        return jnp.where(tp == 0, *orders)

    blocks, blocks_last = whole_plane(own, send), whole_plane(own_last, send_last)
    combine = mixing(route[0], route_weight[0], experts)
    blocks, combine = lax.optimization_barrier((blocks, combine))
    plane = lambda v: lax.all_to_all(v, PLANE, split_axis=0, concat_axis=0, tiled=True)
    mine = plane(blocks)

    down_own = down_master.astype(jnp.bfloat16)
    down_far = swap(down_own, "gr", 1)
    down_own_core, down_far_core = other_core(down_own), other_core(down_far)

    _, width = tokens.shape[1:]
    places = [lax.axis_size(a) for a in FS]
    normed, mix = norm(
        where, tokens.reshape(*places, -1, width), combine.reshape(*places, -1, experts)
    )
    quarters = (down_own, down_far, down_own_core, down_far_core)
    down_out, down_padded = join(where, quarters)

    def along_z(piece):
        below = lax.ppermute(piece, Z, [(1, 0), (2, 1), (0, 3)])
        above = lax.ppermute(piece, Z, [(1, 2), (2, 3), (3, 0)])
        passed = jnp.where(z == 3, below, above)
        far = lax.ppermute(passed, Z, [(3, 2), (0, 1)])
        return piece, below, above, far

    own, below, above, far = along_z(blocks_last)
    pick = lambda a, b, c, d: jnp.where(z < 2, jnp.where(z < 1, a, b), jnp.where(z < 3, c, d))
    raw = jnp.stack([pick(own, below, far, above), pick(below, far, above, own)], axis=1)
    both = plane(raw)
    pieces = [along_z(mine[:, e]) for e in range(experts - 1)] + [(both,)]
    sides = []
    for e in range(experts):
        own = unpack(where, pieces[e])
        sides += [own, other_core(own)]
    outs = last(where, normed, mix, sides, down_padded.reshape(-1, width))
    sums = []
    for color, exchanges in enumerate(COLORS):
        sums.append(Sums(outs[2 * color], outs[2 * color + 1], exchanges))
    for step in range(1, 4):
        for color, exchanges in zip(sums, COLORS):
            color.exchange(*exchanges[step])
    sent = jnp.concatenate([c.block(2, 1).astype(jnp.bfloat16) for c in sums], axis=1)
    came = swap(sent, "fs_0", 1)
    mine = jnp.concatenate([c.block(2, 0) for c in sums], axis=1)
    mixed = added([mine, came]).astype(jnp.bfloat16)[None]
    gate_t, up_t = assemble(where, sides)
    return (jnp.swapaxes(gate_t, 1, 2), jnp.swapaxes(up_t, 1, 2), down_out, mixed)


def solution(mesh):
    split = Mesh(
        mesh.devices.reshape(mesh.shape["gr"], 2, 4, 4, mesh.shape["tp"]),
        ("gr", "fs_0", "fs_1", "fs_2", "tp"),
    )
    in_specs = (
        P(("gr", "tp"), None, None),
        P(None, FS, ("gr", "tp")),
        P(None, FS, ("gr", "tp")),
        P(None, FS, ("gr", "tp")),
        P(FS),
        P(("gr", "tp"), None, None),
        P(("gr", "tp"), None, None),
    )
    out_specs = (P(None, None, FS), P(None, None, FS), P(None, FS, None), P(("gr", "tp"), FS, None))
    return jax.shard_map(
        program, mesh=split, in_specs=in_specs, out_specs=out_specs, check_vma=False
    )
```

```python
import jax
import jax.numpy as jnp
from jax import lax
from jax.experimental import pallas as pl
from jax.experimental.pallas import tpu as pltpu
from jax.sharding import Mesh
from jax.sharding import PartitionSpec as P

FS = ("fs_0", "fs_1", "fs_2")
PLANE = ("fs_1", "fs_2")
Z = ("gr", "fs_0")
UNITS = 256
MIB = 1024 * 1024
LAST_VMEM = 32


COLORS = (
    ((1, 1), (1, 3), (2, 1), (2, 3)),
    ((2, 1), (2, 3), (1, 1), (1, 3)),
    ((1, 3), (1, 1), (2, 3), (2, 1)),
    ((2, 3), (2, 1), (1, 3), (1, 1)),
)


def call(kernel, grid, ins, outs, out_shape, args, flops, nbytes, scratch=(), vmem=60):
    return pl.pallas_call(
        kernel,
        out_shape=out_shape,
        grid_spec=pltpu.PrefetchScalarGridSpec(
            num_scalar_prefetch=1,
            grid=grid,
            in_specs=ins,
            out_specs=outs,
            scratch_shapes=list(scratch),
        ),
        compiler_params=pltpu.CompilerParams(vmem_limit_bytes=vmem * MIB),
        cost_estimate=pl.CostEstimate(
            flops=int(flops), bytes_accessed=int(nbytes), transcendentals=0
        ),
    )(*args)


def whole(shape):
    return pl.BlockSpec(shape, lambda *_: (0,) * len(shape))


def shaped(*shape, dtype=jnp.bfloat16):
    return jax.ShapeDtypeStruct(shape, dtype)


def pack_kernel(where_ref, gate_ref, up_ref, gain_ref, *out_refs):
    depth = gain_ref.shape[1]
    gain = jnp.broadcast_to(gain_ref[...], (128, depth)).T[:, :1]
    rows = jnp.concatenate([gate_ref[0] * gain, up_ref[0] * gain], axis=0)
    cols = rows.astype(jnp.bfloat16).T
    dests, half, lanes = out_refs[-1].shape
    cols = cols.reshape(dests, 2, half, lanes)
    low, high = cols[:, 0], cols[:, 1]
    first = where_ref[1] == 0
    own, send = jnp.where(first, low, high), jnp.where(first, high, low)
    final = pl.program_id(0) == pl.num_programs(0) - 1

    @pl.when(jnp.logical_not(final))
    def _():
        out_refs[0][:, 0] = own
        out_refs[1][:, 0] = send

    @pl.when(final)
    def _():
        out_refs[2][...] = own
        out_refs[3][...] = send


def pack(where, gate, up, gain, dests):
    experts, depth, width = gate.shape
    half = width // dests // 2
    block = pl.BlockSpec((1, depth, width), lambda e, w: (e, 0, 0))
    one = (dests, half, 2 * depth)
    some = pl.BlockSpec((dests, 1, half, 2 * depth), lambda e, w: (0, jnp.minimum(e, experts - 2), 0, 0))
    return call(
        pack_kernel, (experts,), [block, block, whole((1, depth))],
        [some, some, whole(one), whole(one)],
        [shaped(dests, experts - 1, half, 2 * depth)] * 2 + [shaped(*one)] * 2,
        (where, gate, up, gain), 3e9, 6e6,
    )


def unpack_kernel(where_ref, *refs):
    out_ref = refs[-1]
    if len(refs) == 2:
        sources = refs[0].shape[0]
        choices = [[lambda s, part=part: refs[0][s, part] for part in range(2)]]
    else:
        own, below, above, far = refs[:-1]
        sources = own.shape[0]
        pick = ((own, below), (below, far), (far, above), (above, own))
        choices = [[lambda s, ref=ref: ref[s] for ref in two] for two in pick]
    half, lanes = refs[0].shape[-2:]
    left = lax.broadcasted_iota(jnp.int32, (half, lanes), 1) < lanes // 2

    def place(blocks):
        for part, block in enumerate(blocks):
            for pair in range(sources // 2):
                one = block(2 * pair).astype(jnp.float32)
                other = block(2 * pair + 1).astype(jnp.float32)
                crossed = pltpu.roll(jnp.where(left, other, one), lanes // 2, 1)
                start = part * sources * (lanes // 2) + pair * lanes
                at = slice(start, start + lanes)
                out_ref[0, :, at] = jnp.where(left, one, crossed).astype(jnp.bfloat16)
                out_ref[1, :, at] = jnp.where(left, crossed, other).astype(jnp.bfloat16)

    if len(choices) == 1:
        place(choices[0])
    else:
        for plane, blocks in enumerate(choices):
            pl.when(where_ref[0] == plane)(lambda blocks=blocks: place(blocks))


def unpack(where, pieces):
    sources = pieces[0].shape[0]
    half, lanes = pieces[0].shape[-2:]
    shape = (2, half, sources * lanes)
    return call(
        unpack_kernel, (1,), [whole(piece.shape) for piece in pieces], whole(shape),
        shaped(*shape), (where, *pieces), 1e9, 3e6, vmem=12,
    )


def assemble_kernel(where_ref, *refs):
    gate_ref, up_ref = refs[-2:]
    tp = where_ref[1]
    half = refs[0].shape[1]
    for index, ref in enumerate(refs[:-2]):
        side = tp if index % 2 == 0 else 1 - tp
        rows = pl.ds(pl.multiple_of(side * half, 16), half)
        gate_ref[index // 2, rows, :] = ref[0]
        up_ref[index // 2, rows, :] = ref[1]


def assemble(where, sides):
    _, half, width = sides[0].shape
    shape = (len(sides) // 2, 2 * half, width)
    return call(
        assemble_kernel, (1,), [whole(sides[0].shape)] * len(sides),
        [whole(shape)] * 2, [shaped(*shape)] * 2, (where, *sides), 4e9, 11e6, vmem=26,
    )


def join_kernel(where_ref, *refs):
    out_ref, padded_ref = refs[-2:]
    tp, gr = where_ref[1], where_ref[2]
    depth, width = refs[0].shape[1:]
    places = (gr * 2 + tp, (1 - gr) * 2 + tp, gr * 2 + 1 - tp, (1 - gr) * 2 + 1 - tp)
    for ref, place in zip(refs[:-2], places):
        at = pl.ds(pl.multiple_of(place * width, width), width)
        out_ref[0, :, at] = ref[0]
        padded_ref[0, :depth, at] = ref[0]
    rest = padded_ref.shape[1] - depth
    padded_ref[0, depth:, :] = jnp.zeros((rest, padded_ref.shape[2]), jnp.bfloat16)


def join(where, quarters):
    experts, depth, width = quarters[0].shape
    at = lambda e, w: (e, 0, 0)
    return call(
        join_kernel, (experts,), [pl.BlockSpec((1, depth, width), at)] * 4,
        [pl.BlockSpec((1, depth, 4 * width), at), pl.BlockSpec((1, UNITS, 4 * width), at)],
        [shaped(experts, depth, 4 * width), shaped(experts, UNITS, 4 * width)],
        (where, *quarters), 2e9, 8e6, vmem=16,
    )


def norm_kernel(where_ref, tokens_ref, mix_ref, out_ref, mix_out_ref):
    z, x = where_ref[0] % 2, where_ref[4]
    rows = tokens_ref.shape[3]
    for place in range(8):
        zz, xx = z ^ (place % 2), x ^ (place // 2)
        values = tokens_ref[zz, 0, xx].astype(jnp.float32)
        scale = lax.rsqrt(jnp.mean(values * values, axis=-1, keepdims=True) + 1e-06)
        at = slice(place * rows, (place + 1) * rows)
        out_ref[0, at, :] = (values * scale).astype(jnp.bfloat16)
        mix_out_ref[0, at, :] = mix_ref[zz, 0, xx]


def norm(where, tokens, mix):
    zs, ys, xs, rows, width = tokens.shape
    experts = mix.shape[-1]
    block = lambda last: pl.BlockSpec((zs, 1, xs, rows, last), lambda i, w: (0, w[3] ^ i, 0, 0, 0))
    out = lambda last: pl.BlockSpec((1, xs * zs * rows, last), lambda i, w: (i, 0, 0))
    return call(
        norm_kernel, (ys,), [block(width), block(experts)], [out(width), out(experts)],
        [
            shaped(ys, xs * zs * rows, width),
            shaped(ys, xs * zs * rows, experts, dtype=jnp.float32),
        ],
        (where, tokens, mix), 6e9, 17e6, vmem=56,
    )


def fill(where_ref, own_ref, other_ref, gate, up):
    tp = where_ref[1]
    half = own_ref.shape[1]
    for ref, side in ((own_ref, tp), (other_ref, 1 - tp)):
        rows = pl.ds(pl.multiple_of(side * half, 16), half)
        gate[rows, :] = ref[0]
        up[rows, :] = ref[1]
    rest = jnp.zeros((gate.shape[0] - 2 * half, gate.shape[1]), jnp.bfloat16)
    gate[2 * half :, :] = rest
    up[2 * half :, :] = rest


def hidden_of(normed, mix, gate, up):
    dims = (((1,), (1,)), ((), ()))
    gate_act = lax.dot_general(normed, gate, dims, preferred_element_type=jnp.float32)
    up_act = lax.dot_general(normed, up, dims, preferred_element_type=jnp.float32)
    half = 0.5 * gate_act
    return ((half + half * jnp.tanh(half)) * up_act * mix).astype(jnp.bfloat16)


def last_kernel(experts, where_ref, normed_ref, mix_ref, *refs):
    sides = [refs[2 * e : 2 * e + 2] for e in range(experts)]
    down_ref, outs = refs[2 * experts], refs[2 * experts + 1 : -2 * experts]
    scratch = refs[-2 * experts :]
    weights = [scratch[2 * e : 2 * e + 2] for e in range(experts)]
    yy = pl.program_id(0)

    @pl.when(yy == 0)
    def _():
        for side, weight in zip(sides, weights):
            fill(where_ref, *side, *weight)

    hidden = []
    for expert, (gate, up) in enumerate(weights):
        mix = mix_ref[0, :, expert : expert + 1]
        hidden.append(hidden_of(normed_ref[0], mix, gate[...], up[...]))
    rows = jnp.concatenate(hidden, axis=1)
    block = rows.shape[0]
    ys = pl.num_programs(0)
    width = outs[0].shape[1]
    for color, exchanges in enumerate(COLORS):
        at = slice(color * width, (color + 1) * width)
        product = jnp.dot(rows, down_ref[:, at], preferred_element_type=jnp.float32)
        product = product.astype(jnp.bfloat16)
        send_ref, keep_ref = outs[2 * color : 2 * color + 2]
        axis, mask = exchanges[0]
        if axis == 1:
            kept = (yy == 0) | (yy == 4 - mask)
            later = jnp.where((yy == 4 - mask) | (yy == 2), block, 0)
            to = pl.ds(pl.multiple_of(later, block), block)

            @pl.when(kept)
            def _():
                keep_ref[to, :] = product

            @pl.when(jnp.logical_not(kept))
            def _():
                send_ref[to, :] = product

        else:
            part = block // 4
            for xx, ref, k in ((0, keep_ref, 0), (4 - mask, keep_ref, 1), (mask, send_ref, 0), (2, send_ref, 1)):
                to = pl.ds(pl.multiple_of((k * ys + yy) * part, part), part)
                ref[to, :] = product[xx * part : (xx + 1) * part]


def last(where, normed, mix, sides, down):
    ys, rows, width = normed.shape
    experts = len(sides) // 2
    half = (ys * rows // 2, width // len(COLORS))
    at = lambda i, w: (i, 0, 0)
    side = whole(sides[0].shape)
    weight = pltpu.VMEM((UNITS, width), jnp.bfloat16)
    return call(
        lambda *refs: last_kernel(experts, *refs), (ys,),
        [pl.BlockSpec((1, rows, width), at), pl.BlockSpec((1, rows, experts), at)]
        + [side] * (2 * experts) + [whole(down.shape)],
        [whole(half)] * (2 * len(COLORS)), [shaped(*half)] * (2 * len(COLORS)),
        (where, normed, mix, *sides, down), 6 * experts * ys * rows * width * UNITS, 25e6,
        scratch=(weight,) * (2 * experts), vmem=LAST_VMEM,
    )


def swap(array, axis, mask):
    peers = lax.axis_size(axis)
    return lax.ppermute(array, axis, [(i, i ^ mask) for i in range(peers)])


def added(terms):
    total = terms[0].astype(jnp.float32)
    for term in terms[1:]:
        total = total + term.astype(jnp.float32)
    return total


class Sums:
    def __init__(self, send, keep, exchanges):
        axis, mask = exchanges[0]
        self.axes = (axis, *(a for a in (1, 2, 0) if a != axis))
        sizes = [2 if a == 0 else 4 for a in self.axes]
        sizes[0] //= 2
        shape = (*sizes, -1, send.shape[-1])
        came = swap(send, FS[axis], mask).reshape(shape)
        self.offsets = [[0, 1, 2, 3] if a else [0, 1] for a in self.axes]
        self.offsets[0] = [0, 4 - mask] if axis else [0]
        places = [list(range(size)) for size in sizes]
        self.terms = [(keep.reshape(shape), places), (came, [list(p) for p in places])]

    def at(self, dim, index):
        parts = []
        for array, places in self.terms:
            for d, place in enumerate(places):
                if d == dim:
                    array = lax.slice_in_dim(array, place[index], place[index] + 1, axis=d)
                elif len(place) < array.shape[d]:
                    array = lax.slice_in_dim(array, place[0], place[0] + 1, axis=d)
            parts.append(array)
        return added(parts)

    def exchange(self, axis, mask):
        dim = self.axes.index(axis)
        have = self.offsets[dim]
        going, staying = ([mask], [0]) if len(have) == 2 else ([mask, 2], [0, 4 - mask])
        send = [self.at(dim, have.index(o)).astype(jnp.bfloat16) for o in going]
        came = swap(jnp.concatenate(send, axis=dim), FS[axis], mask)
        for _, places in self.terms:
            places[dim] = [places[dim][have.index(o)] for o in staying]
        self.terms.append((came, [list(range(size)) for size in came.shape[:3]]))
        self.offsets[dim] = staying

    def block(self, dim, index):
        total = self.at(dim, index)
        return total.reshape(total.shape[-2:])


def mixing(chosen, weights, experts):
    share = weights / jnp.sum(weights, axis=-1, keepdims=True)
    labels = jnp.arange(experts, dtype=jnp.int32)
    match = (chosen[:, :, None] == labels[None, None, :]).astype(jnp.float32)
    return jnp.sum(share[:, :, None] * match, axis=1)


def program(tokens, gate_master, up_master, down_master, norm_gain, route, route_weight):
    z, tp = lax.axis_index(Z), lax.axis_index("tp")
    where = [z, tp, lax.axis_index("gr"), lax.axis_index("fs_1"), lax.axis_index("fs_2")]
    where = jnp.stack(where).astype(jnp.int32)
    experts = gate_master.shape[0]
    peers = lax.axis_size(PLANE)
    other_core = lambda v: swap(v, "tp", 1)
    gain = norm_gain[None, :]

    own, send, own_last, send_last = pack(where, gate_master, up_master, gain, peers // 2)

    def whole_plane(own, send):
        came = other_core(send)
        orders = [jnp.concatenate(two, axis=0) for two in ((own, came), (came, own))]
        return jnp.where(tp == 0, *orders)

    blocks, blocks_last = whole_plane(own, send), whole_plane(own_last, send_last)
    combine = mixing(route[0], route_weight[0], experts)
    blocks, combine = lax.optimization_barrier((blocks, combine))
    plane = lambda v: lax.all_to_all(v, PLANE, split_axis=0, concat_axis=0, tiled=True)
    mine = plane(blocks)

    down_own = down_master.astype(jnp.bfloat16)
    down_far = swap(down_own, "gr", 1)
    down_own_core, down_far_core = other_core(down_own), other_core(down_far)

    _, width = tokens.shape[1:]
    places = [lax.axis_size(a) for a in FS]
    normed, mix = norm(
        where, tokens.reshape(*places, -1, width), combine.reshape(*places, -1, experts)
    )
    quarters = (down_own, down_far, down_own_core, down_far_core)
    down_out, down_padded = join(where, quarters)

    def along_z(piece):
        below = lax.ppermute(piece, Z, [(1, 0), (2, 1), (0, 3)])
        above = lax.ppermute(piece, Z, [(1, 2), (2, 3), (3, 0)])
        passed = jnp.where(z == 3, below, above)
        far = lax.ppermute(passed, Z, [(3, 2), (0, 1)])
        return piece, below, above, far

    own, below, above, far = along_z(blocks_last)
    pick = lambda a, b, c, d: jnp.where(z < 2, jnp.where(z < 1, a, b), jnp.where(z < 3, c, d))
    raw = jnp.stack([pick(own, below, far, above), pick(below, far, above, own)], axis=1)
    both = plane(raw)
    pieces = [along_z(mine[:, e]) for e in range(experts - 1)] + [(both,)]
    sides = []
    for e in range(experts):
        own = unpack(where, pieces[e])
        sides += [own, other_core(own)]
    outs = last(where, normed, mix, sides, down_padded.reshape(-1, width))
    sums = []
    for color, exchanges in enumerate(COLORS):
        sums.append(Sums(outs[2 * color], outs[2 * color + 1], exchanges))
    for step in range(1, 4):
        for color, exchanges in zip(sums, COLORS):
            color.exchange(*exchanges[step])
    sent = jnp.concatenate([c.block(2, 1).astype(jnp.bfloat16) for c in sums], axis=1)
    came = swap(sent, "fs_0", 1)
    mine = jnp.concatenate([c.block(2, 0) for c in sums], axis=1)
    mixed = added([mine, came]).astype(jnp.bfloat16)[None]
    gate_t, up_t = assemble(where, sides)
    return (jnp.swapaxes(gate_t, 1, 2), jnp.swapaxes(up_t, 1, 2), down_out, mixed)


def solution(mesh):
    split = Mesh(
        mesh.devices.reshape(mesh.shape["gr"], 2, 4, 4, mesh.shape["tp"]),
        ("gr", "fs_0", "fs_1", "fs_2", "tp"),
    )
    in_specs = (
        P(("gr", "tp"), None, None),
        P(None, FS, ("gr", "tp")),
        P(None, FS, ("gr", "tp")),
        P(None, FS, ("gr", "tp")),
        P(FS),
        P(("gr", "tp"), None, None),
        P(("gr", "tp"), None, None),
    )
    out_specs = (P(None, None, FS), P(None, None, FS), P(None, FS, None), P(("gr", "tp"), FS, None))
    return jax.shard_map(
        program, mesh=split, in_specs=in_specs, out_specs=out_specs, check_vma=False
    )
```

```python
import jax
import jax.numpy as jnp
from jax import lax
from jax.experimental import pallas as pl
from jax.experimental.pallas import tpu as pltpu
from jax.sharding import Mesh
from jax.sharding import PartitionSpec as P

FS = ("fs_0", "fs_1", "fs_2")
PLANE = ("fs_1", "fs_2")
Z = ("gr", "fs_0")
UNITS = 256
MIB = 1024 * 1024
LAST_VMEM = 32


COLORS = (
    (((1, 1), (1, 3), (2, 1), (2, 3)), 384),
    (((2, 1), (2, 3), (1, 1), (1, 3)), 384),
    (((1, 3), (1, 1), (2, 3), (2, 1)), 384),
    (((2, 3), (2, 1), (1, 3), (1, 1)), 384),
    (((0, 1), (1, 1), (1, 3), (2, 3), (2, 1)), 256),
    (((0, 1), (2, 1), (2, 3), (1, 3), (1, 1)), 256),
)


def call(kernel, grid, ins, outs, out_shape, args, flops, nbytes, scratch=(), vmem=60):
    return pl.pallas_call(
        kernel,
        out_shape=out_shape,
        grid_spec=pltpu.PrefetchScalarGridSpec(
            num_scalar_prefetch=1,
            grid=grid,
            in_specs=ins,
            out_specs=outs,
            scratch_shapes=list(scratch),
        ),
        compiler_params=pltpu.CompilerParams(vmem_limit_bytes=vmem * MIB),
        cost_estimate=pl.CostEstimate(
            flops=int(flops), bytes_accessed=int(nbytes), transcendentals=0
        ),
    )(*args)


def whole(shape):
    return pl.BlockSpec(shape, lambda *_: (0,) * len(shape))


def shaped(*shape, dtype=jnp.bfloat16):
    return jax.ShapeDtypeStruct(shape, dtype)


def pack_kernel(where_ref, gate_ref, up_ref, gain_ref, own_ref, send_ref):
    depth = gain_ref.shape[1]
    gain = jnp.broadcast_to(gain_ref[...], (128, depth)).T[:, :1]
    rows = jnp.concatenate([gate_ref[0] * gain, up_ref[0] * gain], axis=0)
    cols = rows.astype(jnp.bfloat16).T
    dests, _, half, lanes = own_ref.shape
    cols = cols.reshape(dests, 2, half, lanes)
    low, high = cols[:, 0], cols[:, 1]
    first = where_ref[1] == 0
    own_ref[:, 0] = jnp.where(first, low, high)
    send_ref[:, 0] = jnp.where(first, high, low)


def pack(where, gate, up, gain, dests):
    experts, depth, width = gate.shape
    half = width // dests // 2
    block = pl.BlockSpec((1, depth, width), lambda e, w: (e, 0, 0))
    out = pl.BlockSpec((dests, 1, half, 2 * depth), lambda e, w: (0, e, 0, 0))
    return call(
        pack_kernel, (experts,), [block, block, whole((1, depth))], [out] * 2,
        [shaped(dests, experts, half, 2 * depth)] * 2, (where, gate, up, gain), 3e9, 6e6,
    )


def unpack_kernel(where_ref, own_ref, down_ref, up_ref, far_ref, out_ref):
    z = where_ref[0]
    sources, half, lanes = own_ref.shape
    left = lax.broadcasted_iota(jnp.int32, (half, lanes), 1) < lanes // 2
    pick = ((own_ref, down_ref, far_ref, up_ref), (down_ref, far_ref, up_ref, own_ref))
    for plane in range(4):

        @pl.when(z == plane)
        def _():
            for part in range(2):
                ref = pick[part][plane]
                for pair in range(sources // 2):
                    one = ref[2 * pair].astype(jnp.float32)
                    other = ref[2 * pair + 1].astype(jnp.float32)
                    crossed = pltpu.roll(jnp.where(left, other, one), lanes // 2, 1)
                    start = part * sources * (lanes // 2) + pair * lanes
                    at = slice(start, start + lanes)
                    out_ref[0, :, at] = jnp.where(left, one, crossed).astype(jnp.bfloat16)
                    out_ref[1, :, at] = jnp.where(left, crossed, other).astype(jnp.bfloat16)


def unpack(where, pieces):
    sources, half, lanes = pieces[0].shape
    shape = (2, half, sources * lanes)
    return call(
        unpack_kernel, (1,), [whole(pieces[0].shape)] * 4, whole(shape),
        shaped(*shape), (where, *pieces), 1e9, 3e6, vmem=12,
    )


def assemble_kernel(where_ref, *refs):
    gate_ref, up_ref = refs[-2:]
    tp = where_ref[1]
    half = refs[0].shape[1]
    for index, ref in enumerate(refs[:-2]):
        side = tp if index % 2 == 0 else 1 - tp
        rows = pl.ds(pl.multiple_of(side * half, 16), half)
        gate_ref[index // 2, rows, :] = ref[0]
        up_ref[index // 2, rows, :] = ref[1]


def assemble(where, sides):
    _, half, width = sides[0].shape
    shape = (len(sides) // 2, 2 * half, width)
    return call(
        assemble_kernel, (1,), [whole(sides[0].shape)] * len(sides),
        [whole(shape)] * 2, [shaped(*shape)] * 2, (where, *sides), 4e9, 11e6, vmem=26,
    )


def join_kernel(where_ref, *refs):
    out_ref, padded_ref = refs[-2:]
    tp, gr = where_ref[1], where_ref[2]
    depth, width = refs[0].shape[1:]
    places = (gr * 2 + tp, (1 - gr) * 2 + tp, gr * 2 + 1 - tp, (1 - gr) * 2 + 1 - tp)
    for ref, place in zip(refs[:-2], places):
        at = pl.ds(pl.multiple_of(place * width, width), width)
        out_ref[0, :, at] = ref[0]
        padded_ref[0, :depth, at] = ref[0]
    rest = padded_ref.shape[1] - depth
    padded_ref[0, depth:, :] = jnp.zeros((rest, padded_ref.shape[2]), jnp.bfloat16)


def join(where, quarters):
    experts, depth, width = quarters[0].shape
    at = lambda e, w: (e, 0, 0)
    return call(
        join_kernel, (experts,), [pl.BlockSpec((1, depth, width), at)] * 4,
        [pl.BlockSpec((1, depth, 4 * width), at), pl.BlockSpec((1, UNITS, 4 * width), at)],
        [shaped(experts, depth, 4 * width), shaped(experts, UNITS, 4 * width)],
        (where, *quarters), 2e9, 8e6, vmem=16,
    )


def norm_kernel(where_ref, tokens_ref, mix_ref, out_ref, mix_out_ref):
    z, x = where_ref[0] % 2, where_ref[4]
    rows = tokens_ref.shape[3]
    for place in range(8):
        zz, xx = z ^ (place % 2), x ^ (place // 2)
        values = tokens_ref[zz, 0, xx].astype(jnp.float32)
        scale = lax.rsqrt(jnp.mean(values * values, axis=-1, keepdims=True) + 1e-06)
        at = slice(place * rows, (place + 1) * rows)
        out_ref[0, at, :] = (values * scale).astype(jnp.bfloat16)
        mix_out_ref[0, at, :] = mix_ref[zz, 0, xx]


def norm(where, tokens, mix):
    zs, ys, xs, rows, width = tokens.shape
    experts = mix.shape[-1]
    block = lambda last: pl.BlockSpec((zs, 1, xs, rows, last), lambda i, w: (0, w[3] ^ i, 0, 0, 0))
    out = lambda last: pl.BlockSpec((1, xs * zs * rows, last), lambda i, w: (i, 0, 0))
    return call(
        norm_kernel, (ys,), [block(width), block(experts)], [out(width), out(experts)],
        [
            shaped(ys, xs * zs * rows, width),
            shaped(ys, xs * zs * rows, experts, dtype=jnp.float32),
        ],
        (where, tokens, mix), 6e9, 17e6,
    )


def fill(where_ref, own_ref, other_ref, gate, up):
    tp = where_ref[1]
    half = own_ref.shape[1]
    for ref, side in ((own_ref, tp), (other_ref, 1 - tp)):
        rows = pl.ds(pl.multiple_of(side * half, 16), half)
        gate[rows, :] = ref[0]
        up[rows, :] = ref[1]
    rest = jnp.zeros((gate.shape[0] - 2 * half, gate.shape[1]), jnp.bfloat16)
    gate[2 * half :, :] = rest
    up[2 * half :, :] = rest


def hidden_of(normed, mix, gate, up):
    dims = (((1,), (1,)), ((), ()))
    gate_act = lax.dot_general(normed, gate, dims, preferred_element_type=jnp.float32)
    up_act = lax.dot_general(normed, up, dims, preferred_element_type=jnp.float32)
    return (gate_act / (1.0 + jnp.exp(-gate_act)) * up_act * mix).astype(jnp.bfloat16)


def hidden_kernel(expert, where_ref, normed_ref, mix_ref, own_ref, other_ref, out_ref, gate, up):
    @pl.when(pl.program_id(0) == 0)
    def _():
        fill(where_ref, own_ref, other_ref, gate, up)

    mix = mix_ref[0, :, expert : expert + 1]
    out_ref[0] = hidden_of(normed_ref[0], mix, gate[...], up[...])


def hidden_units(where, normed, mix, own, other, expert):
    groups, rows, width = normed.shape
    at = lambda g, w: (g, 0, 0)
    side = whole(own.shape)
    weight = pltpu.VMEM((UNITS, width), jnp.bfloat16)
    return call(
        lambda *refs: hidden_kernel(expert, *refs), (groups,),
        [pl.BlockSpec((1, rows, width), at), pl.BlockSpec((1, rows, mix.shape[-1]), at), side, side],
        pl.BlockSpec((1, rows, UNITS), at), shaped(groups, rows, UNITS),
        (where, normed, mix, own, other), 4 * groups * rows * width * UNITS, 12e6,
        scratch=(weight, weight), vmem=48,
    )


def last_kernel(where_ref, normed_ref, mix_ref, early_ref, *refs):
    sides, down_ref = (refs[0:2], refs[2:4]), refs[4]
    outs, weights = refs[5:-4], (refs[-4:-2], refs[-2:])
    yy = pl.program_id(0)

    @pl.when(yy == 0)
    def _():
        for side, weight in zip(sides, weights):
            fill(where_ref, *side, *weight)

    hidden = [early_ref[0]]
    for expert, (gate, up) in enumerate(weights, 1):
        mix = mix_ref[0, :, expert : expert + 1]
        hidden.append(hidden_of(normed_ref[0], mix, gate[...], up[...]))
    rows = jnp.concatenate(hidden, axis=1)
    block = rows.shape[0]
    ys = pl.num_programs(0)
    start, place = 0, 0
    for color in range(0, len(COLORS), 2):
        columns = sum(width for _, width in COLORS[color : color + 2])
        at = slice(start, start + columns)
        start += columns
        both = jnp.dot(rows, down_ref[:, at], preferred_element_type=jnp.float32)
        both = both.astype(jnp.bfloat16)
        used = 0
        for exchanges, width in COLORS[color : color + 2]:
            product = both[:, used : used + width]
            used += width
            axis, mask = exchanges[0]
            count = 3 if axis else 2
            send_ref, keep_refs = outs[place], outs[place + 1 : place + count]
            place += count
            moves = ((0, keep_refs[0], 0), (4 - mask, keep_refs[-1], 0), (mask, send_ref, 0), (2, send_ref, 1))
            if axis == 1:
                for at_y, ref, k in moves:

                    @pl.when(yy == at_y)
                    def _():
                        ref[k * block : (k + 1) * block, :] = product

            elif axis == 2:
                part = block // 4
                for xx, ref, k in moves:
                    to = pl.ds(pl.multiple_of((k * ys + yy) * part, part), part)
                    ref[to, :] = product[xx * part : (xx + 1) * part]
            else:
                part = block // 8
                for index in range(8):
                    ref = send_ref if index % 2 else keep_refs[0]
                    to = pl.ds(pl.multiple_of((yy * 4 + index // 2) * part, part), part)
                    ref[to, :] = product[index * part : (index + 1) * part]


def last(where, normed, mix, early, sides, down):
    ys, rows, width = normed.shape
    outs = []
    for exchanges, columns in COLORS:
        half, quarter = (ys * rows // 2, columns), (ys * rows // 4, columns)
        outs += [half, quarter, quarter] if exchanges[0][0] else [half, half]
    at = lambda i, w: (i, 0, 0)
    side = whole(sides[0].shape)
    weight = pltpu.VMEM((UNITS, width), jnp.bfloat16)
    return call(
        last_kernel, (ys,),
        [pl.BlockSpec((1, rows, width), at), pl.BlockSpec((1, rows, mix.shape[-1]), at)]
        + [pl.BlockSpec((1, rows, UNITS), at)] + [side] * 4 + [whole(down.shape)],
        [whole(out) for out in outs], [shaped(*out) for out in outs],
        (where, normed, mix, early, *sides, down), 14 * ys * rows * width * UNITS, 25e6,
        scratch=(weight,) * 4, vmem=LAST_VMEM,
    )


def swap(array, axis, mask):
    peers = lax.axis_size(axis)
    return lax.ppermute(array, axis, [(i, i ^ mask) for i in range(peers)])


def added(terms):
    total = terms[0].astype(jnp.float32)
    for term in terms[1:]:
        total = total + term.astype(jnp.float32)
    return total


class Sums:
    def __init__(self, send, keeps, exchanges):
        axis, mask = exchanges[0]
        self.axes = (axis, *(a for a in (1, 2, 0) if a != axis))
        sizes = [2 if a == 0 else 4 for a in self.axes]
        sizes[0] //= 2
        shape = (*sizes, -1, send.shape[-1])
        came = swap(send, FS[axis], mask).reshape(shape)
        self.offsets = [[0, 1, 2, 3] if a else [0, 1] for a in self.axes]
        self.offsets[0] = [0, 4 - mask] if axis else [0]
        places = [list(range(size)) for size in sizes]
        keeps = [keep.reshape(1, *shape[1:]) for keep in keeps]
        self.terms = [(keeps, places), (came, [list(p) for p in places])]

    def at(self, dim, index):
        parts = []
        for array, places in self.terms:
            for d, place in enumerate(places):
                if isinstance(array, list):
                    array = array[place[index if dim == 0 else 0]]
                elif d == dim:
                    array = lax.slice_in_dim(array, place[index], place[index] + 1, axis=d)
                elif len(place) < array.shape[d]:
                    array = lax.slice_in_dim(array, place[0], place[0] + 1, axis=d)
            parts.append(array)
        return added(parts)

    def exchange(self, axis, mask):
        dim = self.axes.index(axis)
        have = self.offsets[dim]
        going, staying = ([mask], [0]) if len(have) == 2 else ([mask, 2], [0, 4 - mask])
        send = [self.at(dim, have.index(o)).astype(jnp.bfloat16) for o in going]
        came = swap(jnp.concatenate(send, axis=dim), FS[axis], mask)
        for _, places in self.terms:
            places[dim] = [places[dim][have.index(o)] for o in staying]
        self.terms.append((came, [list(range(size)) for size in came.shape[:3]]))
        self.offsets[dim] = staying

    def block(self, dim, index):
        total = self.at(dim, index)
        return total.reshape(total.shape[-2:])


def mixing(chosen, weights, experts):
    share = weights / jnp.sum(weights, axis=-1, keepdims=True)
    labels = jnp.arange(experts, dtype=jnp.int32)
    match = (chosen[:, :, None] == labels[None, None, :]).astype(jnp.float32)
    return jnp.sum(share[:, :, None] * match, axis=1)


def program(tokens, gate_master, up_master, down_master, norm_gain, route, route_weight):
    z, tp = lax.axis_index(Z), lax.axis_index("tp")
    where = [z, tp, lax.axis_index("gr"), lax.axis_index("fs_1"), lax.axis_index("fs_2")]
    where = jnp.stack(where).astype(jnp.int32)
    experts = gate_master.shape[0]
    peers = lax.axis_size(PLANE)
    other_core = lambda v: swap(v, "tp", 1)
    gain = norm_gain[None, :]

    own, send = pack(where, gate_master, up_master, gain, peers // 2)
    came = other_core(send)
    blocks = jnp.where(
        tp == 0, jnp.concatenate([own, came], axis=0), jnp.concatenate([came, own], axis=0)
    )
    combine = mixing(route[0], route_weight[0], experts)
    blocks, combine = lax.optimization_barrier((blocks, combine))
    mine = lax.all_to_all(blocks, PLANE, split_axis=0, concat_axis=0, tiled=True)

    down_own = down_master.astype(jnp.bfloat16)
    down_far = swap(down_own, "gr", 1)
    down_own_core = other_core(down_own)
    down_far_core = other_core(down_far)

    count, width = tokens.shape[1:]
    places = [lax.axis_size(a) for a in FS]
    normed, mix = norm(
        where, tokens.reshape(*places, -1, width), combine.reshape(*places, -1, experts)
    )
    quarters = (down_own, down_far, down_own_core, down_far_core)
    down_out, down_padded = join(where, quarters)
    mine, normed = lax.optimization_barrier((mine, normed))

    sides = []
    for e in range(experts):
        piece = mine[:, e]
        below = lax.ppermute(piece, Z, [(1, 0), (2, 1), (0, 3)])
        above = lax.ppermute(piece, Z, [(1, 2), (2, 3), (3, 0)])
        passed = jnp.where(z == 3, below, above)
        far = lax.ppermute(passed, Z, [(3, 2), (0, 1)])
        own = unpack(where, (piece, below, above, far))
        sides += [own, other_core(own)]
    early = hidden_units(where, normed, mix, sides[0], sides[1], 0)
    outs = last(where, normed, mix, early, sides[2:], down_padded.reshape(-1, width))
    sums, place = [], 0
    for exchanges, _ in COLORS:
        count = 3 if exchanges[0][0] else 2
        sums.append(Sums(outs[place], outs[place + 1 : place + count], exchanges))
        place += count
    for step in range(1, 5):
        for color, (exchanges, _) in enumerate(COLORS):
            if step < len(exchanges):
                sums[color].exchange(*exchanges[step])
    columns = []
    for pair in (sums[0:2], sums[2:4]):
        sent = jnp.concatenate([c.block(2, 1).astype(jnp.bfloat16) for c in pair], axis=1)
        came = swap(sent, "fs_0", 1)
        columns.append(added([jnp.concatenate([c.block(2, 0) for c in pair], axis=1), came]))
    columns += [c.block(0, 0) for c in sums[4:]]
    mixed = jnp.concatenate(columns, axis=1).astype(jnp.bfloat16)[None]
    gate_t, up_t = assemble(where, sides)
    return (jnp.swapaxes(gate_t, 1, 2), jnp.swapaxes(up_t, 1, 2), down_out, mixed)


def solution(mesh):
    split = Mesh(
        mesh.devices.reshape(mesh.shape["gr"], 2, 4, 4, mesh.shape["tp"]),
        ("gr", "fs_0", "fs_1", "fs_2", "tp"),
    )
    in_specs = (
        P(("gr", "tp"), None, None),
        P(None, FS, ("gr", "tp")),
        P(None, FS, ("gr", "tp")),
        P(None, FS, ("gr", "tp")),
        P(FS),
        P(("gr", "tp"), None, None),
        P(("gr", "tp"), None, None),
    )
    out_specs = (P(None, None, FS), P(None, None, FS), P(None, FS, None), P(("gr", "tp"), FS, None))
    return jax.shard_map(
        program, mesh=split, in_specs=in_specs, out_specs=out_specs, check_vma=False
    )
```

```python
import jax
import jax.numpy as jnp
from jax import lax
from jax.experimental import pallas as pl
from jax.experimental.pallas import tpu as pltpu
from jax.sharding import Mesh
from jax.sharding import PartitionSpec as P

FS = ("fs_0", "fs_1", "fs_2")
PLANE = ("fs_1", "fs_2")
Z = ("gr", "fs_0")
UNITS = 256
MIB = 1024 * 1024
LAST_VMEM = 32


COLORS = (
    ((1, 1), (1, 3), (2, 1), (2, 3)),
    ((2, 1), (2, 3), (1, 1), (1, 3)),
    ((1, 3), (1, 1), (2, 3), (2, 1)),
    ((2, 3), (2, 1), (1, 3), (1, 1)),
)


def call(kernel, grid, ins, outs, out_shape, args, flops, nbytes, scratch=(), vmem=60):
    return pl.pallas_call(
        kernel,
        out_shape=out_shape,
        grid_spec=pltpu.PrefetchScalarGridSpec(
            num_scalar_prefetch=1,
            grid=grid,
            in_specs=ins,
            out_specs=outs,
            scratch_shapes=list(scratch),
        ),
        compiler_params=pltpu.CompilerParams(vmem_limit_bytes=vmem * MIB),
        cost_estimate=pl.CostEstimate(
            flops=int(flops), bytes_accessed=int(nbytes), transcendentals=0
        ),
    )(*args)


def whole(shape):
    return pl.BlockSpec(shape, lambda *_: (0,) * len(shape))


def shaped(*shape, dtype=jnp.bfloat16):
    return jax.ShapeDtypeStruct(shape, dtype)


def pack_kernel(where_ref, gate_ref, up_ref, gain_ref, own_ref, send_ref):
    depth = gain_ref.shape[1]
    gain = jnp.broadcast_to(gain_ref[...], (128, depth)).T[:, :1]
    rows = jnp.concatenate([gate_ref[0] * gain, up_ref[0] * gain], axis=0)
    cols = rows.astype(jnp.bfloat16).T
    dests, _, half, lanes = own_ref.shape
    cols = cols.reshape(dests, 2, half, lanes)
    low, high = cols[:, 0], cols[:, 1]
    first = where_ref[1] == 0
    own_ref[:, 0] = jnp.where(first, low, high)
    send_ref[:, 0] = jnp.where(first, high, low)


def pack(where, gate, up, gain, dests):
    experts, depth, width = gate.shape
    half = width // dests // 2
    block = pl.BlockSpec((1, depth, width), lambda e, w: (e, 0, 0))
    out = pl.BlockSpec((dests, 1, half, 2 * depth), lambda e, w: (0, e, 0, 0))
    return call(
        pack_kernel, (experts,), [block, block, whole((1, depth))], [out] * 2,
        [shaped(dests, experts, half, 2 * depth)] * 2, (where, gate, up, gain), 3e9, 6e6,
    )


def unpack_kernel(where_ref, *refs):
    own_ref, out_ref = refs[0], refs[-1]
    z = where_ref[0]
    sources, half, lanes = own_ref.shape
    left = lax.broadcasted_iota(jnp.int32, (half, lanes), 1) < lanes // 2
    if len(refs) == 5:
        _, below, above, far = refs[:-1]
        pick = ((own_ref, below, far, above), (below, far, above, own_ref))
    else:
        _, outer, inner = refs[:-1]
        pick = ((own_ref, inner, outer, outer), (outer, outer, inner, own_ref))
    for plane in range(4):

        @pl.when(z == plane)
        def _():
            for part in range(2):
                ref = pick[part][plane]
                for pair in range(sources // 2):
                    one = ref[2 * pair].astype(jnp.float32)
                    other = ref[2 * pair + 1].astype(jnp.float32)
                    crossed = pltpu.roll(jnp.where(left, other, one), lanes // 2, 1)
                    start = part * sources * (lanes // 2) + pair * lanes
                    at = slice(start, start + lanes)
                    out_ref[0, :, at] = jnp.where(left, one, crossed).astype(jnp.bfloat16)
                    out_ref[1, :, at] = jnp.where(left, crossed, other).astype(jnp.bfloat16)


def unpack(where, pieces):
    sources, half, lanes = pieces[0].shape
    shape = (2, half, sources * lanes)
    return call(
        unpack_kernel, (1,), [whole(pieces[0].shape)] * len(pieces), whole(shape),
        shaped(*shape), (where, *pieces), 1e9, 3e6, vmem=12,
    )


def assemble_kernel(where_ref, *refs):
    gate_ref, up_ref = refs[-2:]
    tp = where_ref[1]
    half = refs[0].shape[1]
    for index, ref in enumerate(refs[:-2]):
        side = tp if index % 2 == 0 else 1 - tp
        rows = pl.ds(pl.multiple_of(side * half, 16), half)
        gate_ref[index // 2, rows, :] = ref[0]
        up_ref[index // 2, rows, :] = ref[1]


def assemble(where, sides):
    _, half, width = sides[0].shape
    shape = (len(sides) // 2, 2 * half, width)
    return call(
        assemble_kernel, (1,), [whole(sides[0].shape)] * len(sides),
        [whole(shape)] * 2, [shaped(*shape)] * 2, (where, *sides), 4e9, 11e6, vmem=26,
    )


def join_kernel(where_ref, *refs):
    out_ref, padded_ref = refs[-2:]
    tp, gr = where_ref[1], where_ref[2]
    depth, width = refs[0].shape[1:]
    places = (gr * 2 + tp, (1 - gr) * 2 + tp, gr * 2 + 1 - tp, (1 - gr) * 2 + 1 - tp)
    for ref, place in zip(refs[:-2], places):
        at = pl.ds(pl.multiple_of(place * width, width), width)
        out_ref[0, :, at] = ref[0]
        padded_ref[0, :depth, at] = ref[0]
    rest = padded_ref.shape[1] - depth
    padded_ref[0, depth:, :] = jnp.zeros((rest, padded_ref.shape[2]), jnp.bfloat16)


def join(where, quarters):
    experts, depth, width = quarters[0].shape
    at = lambda e, w: (e, 0, 0)
    return call(
        join_kernel, (experts,), [pl.BlockSpec((1, depth, width), at)] * 4,
        [pl.BlockSpec((1, depth, 4 * width), at), pl.BlockSpec((1, UNITS, 4 * width), at)],
        [shaped(experts, depth, 4 * width), shaped(experts, UNITS, 4 * width)],
        (where, *quarters), 2e9, 8e6, vmem=16,
    )


def norm_kernel(where_ref, tokens_ref, mix_ref, out_ref, mix_out_ref):
    z, x = where_ref[0] % 2, where_ref[4]
    rows = tokens_ref.shape[3]
    for place in range(8):
        zz, xx = z ^ (place % 2), x ^ (place // 2)
        values = tokens_ref[zz, 0, xx].astype(jnp.float32)
        scale = lax.rsqrt(jnp.mean(values * values, axis=-1, keepdims=True) + 1e-06)
        at = slice(place * rows, (place + 1) * rows)
        out_ref[0, at, :] = (values * scale).astype(jnp.bfloat16)
        mix_out_ref[0, at, :] = mix_ref[zz, 0, xx]


def norm(where, tokens, mix):
    zs, ys, xs, rows, width = tokens.shape
    experts = mix.shape[-1]
    block = lambda last: pl.BlockSpec((zs, 1, xs, rows, last), lambda i, w: (0, w[3] ^ i, 0, 0, 0))
    out = lambda last: pl.BlockSpec((1, xs * zs * rows, last), lambda i, w: (i, 0, 0))
    return call(
        norm_kernel, (ys,), [block(width), block(experts)], [out(width), out(experts)],
        [
            shaped(ys, xs * zs * rows, width),
            shaped(ys, xs * zs * rows, experts, dtype=jnp.float32),
        ],
        (where, tokens, mix), 6e9, 17e6,
    )


def fill(where_ref, own_ref, other_ref, gate, up):
    tp = where_ref[1]
    half = own_ref.shape[1]
    for ref, side in ((own_ref, tp), (other_ref, 1 - tp)):
        rows = pl.ds(pl.multiple_of(side * half, 16), half)
        gate[rows, :] = ref[0]
        up[rows, :] = ref[1]
    rest = jnp.zeros((gate.shape[0] - 2 * half, gate.shape[1]), jnp.bfloat16)
    gate[2 * half :, :] = rest
    up[2 * half :, :] = rest


def hidden_of(normed, mix, gate, up):
    dims = (((1,), (1,)), ((), ()))
    gate_act = lax.dot_general(normed, gate, dims, preferred_element_type=jnp.float32)
    up_act = lax.dot_general(normed, up, dims, preferred_element_type=jnp.float32)
    return (gate_act / (1.0 + jnp.exp(-gate_act)) * up_act * mix).astype(jnp.bfloat16)


def hidden_kernel(expert, where_ref, normed_ref, mix_ref, own_ref, other_ref, out_ref, gate, up):
    @pl.when(pl.program_id(0) == 0)
    def _():
        fill(where_ref, own_ref, other_ref, gate, up)

    mix = mix_ref[0, :, expert : expert + 1]
    out_ref[0] = hidden_of(normed_ref[0], mix, gate[...], up[...])


def hidden_units(where, normed, mix, own, other, expert):
    groups, rows, width = normed.shape
    at = lambda g, w: (g, 0, 0)
    side = whole(own.shape)
    weight = pltpu.VMEM((UNITS, width), jnp.bfloat16)
    return call(
        lambda *refs: hidden_kernel(expert, *refs), (groups,),
        [pl.BlockSpec((1, rows, width), at), pl.BlockSpec((1, rows, mix.shape[-1]), at), side, side],
        pl.BlockSpec((1, rows, UNITS), at), shaped(groups, rows, UNITS),
        (where, normed, mix, own, other), 4 * groups * rows * width * UNITS, 12e6,
        scratch=(weight, weight), vmem=48,
    )


def last_kernel(where_ref, normed_ref, mix_ref, early_ref, *refs):
    sides, down_ref = (refs[0:2], refs[2:4]), refs[4]
    outs, weights = refs[5:-4], (refs[-4:-2], refs[-2:])
    yy = pl.program_id(0)

    @pl.when(yy == 0)
    def _():
        for side, weight in zip(sides, weights):
            fill(where_ref, *side, *weight)

    hidden = [early_ref[0]]
    for expert, (gate, up) in enumerate(weights, 1):
        mix = mix_ref[0, :, expert : expert + 1]
        hidden.append(hidden_of(normed_ref[0], mix, gate[...], up[...]))
    rows = jnp.concatenate(hidden, axis=1)
    block = rows.shape[0]
    ys = pl.num_programs(0)
    width = outs[0].shape[1]
    for color, exchanges in enumerate(COLORS):
        at = slice(color * width, (color + 1) * width)
        product = jnp.dot(rows, down_ref[:, at], preferred_element_type=jnp.float32)
        product = product.astype(jnp.bfloat16)
        send_ref, keep_refs = outs[3 * color], outs[3 * color + 1 : 3 * color + 3]
        axis, mask = exchanges[0]
        if axis == 1:
            for at_y, ref, start in (
                (0, keep_refs[0], 0),
                (4 - mask, keep_refs[1], 0),
                (mask, send_ref, 0),
                (2, send_ref, block),
            ):

                @pl.when(yy == at_y)
                def _():
                    ref[start : start + block, :] = product

        else:
            part = block // 4
            for xx, ref, k in (
                (0, keep_refs[0], 0),
                (4 - mask, keep_refs[1], 0),
                (mask, send_ref, 0),
                (2, send_ref, 1),
            ):
                to = pl.ds(pl.multiple_of((k * ys + yy) * part, part), part)
                ref[to, :] = product[xx * part : (xx + 1) * part]


def last(where, normed, mix, early, sides, down):
    ys, rows, width = normed.shape
    quarter = (ys * rows // 4, width // len(COLORS))
    outs = [(2 * quarter[0], quarter[1]), quarter, quarter] * len(COLORS)
    at = lambda i, w: (i, 0, 0)
    side = whole(sides[0].shape)
    weight = pltpu.VMEM((UNITS, width), jnp.bfloat16)
    return call(
        last_kernel, (ys,),
        [pl.BlockSpec((1, rows, width), at), pl.BlockSpec((1, rows, mix.shape[-1]), at)]
        + [pl.BlockSpec((1, rows, UNITS), at)] + [side] * 4 + [whole(down.shape)],
        [whole(out) for out in outs], [shaped(*out) for out in outs],
        (where, normed, mix, early, *sides, down), 14 * ys * rows * width * UNITS, 25e6,
        scratch=(weight,) * 4, vmem=LAST_VMEM,
    )


def swap(array, axis, mask):
    peers = lax.axis_size(axis)
    return lax.ppermute(array, axis, [(i, i ^ mask) for i in range(peers)])


def added(terms):
    total = terms[0].astype(jnp.float32)
    for term in terms[1:]:
        total = total + term.astype(jnp.float32)
    return total


class Sums:
    def __init__(self, send, keeps, exchanges):
        axis, mask = exchanges[0]
        self.axes = (axis, *(a for a in (1, 2, 0) if a != axis))
        sizes = [2 if a == 0 else 4 for a in self.axes]
        sizes[0] //= 2
        shape = (*sizes, -1, send.shape[-1])
        came = swap(send, FS[axis], mask).reshape(shape)
        self.offsets = [[0, 1, 2, 3] if a else [0, 1] for a in self.axes]
        self.offsets[0] = [0, 4 - mask] if axis else [0]
        places = [list(range(size)) for size in sizes]
        keeps = [keep.reshape(1, *shape[1:]) for keep in keeps]
        self.terms = [(keeps, places), (came, [list(p) for p in places])]

    def at(self, dim, index):
        parts = []
        for array, places in self.terms:
            for d, place in enumerate(places):
                if isinstance(array, list):
                    array = array[place[index if dim == 0 else 0]]
                elif d == dim:
                    array = lax.slice_in_dim(array, place[index], place[index] + 1, axis=d)
                elif len(place) < array.shape[d]:
                    array = lax.slice_in_dim(array, place[0], place[0] + 1, axis=d)
            parts.append(array)
        return added(parts)

    def exchange(self, axis, mask):
        dim = self.axes.index(axis)
        have = self.offsets[dim]
        going, staying = ([mask], [0]) if len(have) == 2 else ([mask, 2], [0, 4 - mask])
        send = [self.at(dim, have.index(o)).astype(jnp.bfloat16) for o in going]
        came = swap(jnp.concatenate(send, axis=dim), FS[axis], mask)
        for _, places in self.terms:
            places[dim] = [places[dim][have.index(o)] for o in staying]
        self.terms.append((came, [list(range(size)) for size in came.shape[:3]]))
        self.offsets[dim] = staying

    def block(self, dim, index):
        total = self.at(dim, index)
        return total.reshape(total.shape[-2:])


def mixing(chosen, weights, experts):
    share = weights / jnp.sum(weights, axis=-1, keepdims=True)
    labels = jnp.arange(experts, dtype=jnp.int32)
    match = (chosen[:, :, None] == labels[None, None, :]).astype(jnp.float32)
    return jnp.sum(share[:, :, None] * match, axis=1)


def program(tokens, gate_master, up_master, down_master, norm_gain, route, route_weight):
    z, tp = lax.axis_index(Z), lax.axis_index("tp")
    where = [z, tp, lax.axis_index("gr"), lax.axis_index("fs_1"), lax.axis_index("fs_2")]
    where = jnp.stack(where).astype(jnp.int32)
    experts = gate_master.shape[0]
    peers = lax.axis_size(PLANE)
    other_core = lambda v: swap(v, "tp", 1)
    gain = norm_gain[None, :]

    own, send = pack(where, gate_master, up_master, gain, peers // 2)
    came = other_core(send)
    blocks = jnp.where(
        tp == 0, jnp.concatenate([own, came], axis=0), jnp.concatenate([came, own], axis=0)
    )
    combine = mixing(route[0], route_weight[0], experts)
    blocks, combine = lax.optimization_barrier((blocks, combine))
    mine = lax.all_to_all(blocks, PLANE, split_axis=0, concat_axis=0, tiled=True)

    down_own = down_master.astype(jnp.bfloat16)
    down_far = swap(down_own, "gr", 1)
    down_own_core = other_core(down_own)
    down_far_core = other_core(down_far)

    _, width = tokens.shape[1:]
    places = [lax.axis_size(a) for a in FS]
    normed, mix = norm(
        where, tokens.reshape(*places, -1, width), combine.reshape(*places, -1, experts)
    )
    quarters = (down_own, down_far, down_own_core, down_far_core)
    down_out, down_padded = join(where, quarters)
    mine, normed = lax.optimization_barrier((mine, normed))

    sides = []
    for e in range(experts):
        piece = mine[:, e]
        forwarded = e < experts - 1
        outer = [(1, 0), (2, 1), (0, 3)] if forwarded else [(1, 0), (2, 3), (0, 2), (3, 1)]
        inner = [(1, 2), (2, 3), (3, 0)] if forwarded else [(1, 2), (2, 1)]
        pieces = [piece, lax.ppermute(piece, Z, outer)]
        pieces.append(lax.ppermute(piece, Z, inner))
        if forwarded:
            passed = jnp.where(z == 3, *pieces[1:])
            pieces.append(lax.ppermute(passed, Z, [(3, 2), (0, 1)]))
        own = unpack(where, pieces)
        sides += [own, other_core(own)]
    early = hidden_units(where, normed, mix, sides[0], sides[1], 0)
    outs = last(where, normed, mix, early, sides[2:], down_padded.reshape(-1, width))
    sums = []
    for color, exchanges in enumerate(COLORS):
        sums.append(Sums(outs[3 * color], outs[3 * color + 1 : 3 * color + 3], exchanges))
    for step in range(1, 4):
        for color, exchanges in zip(sums, COLORS):
            color.exchange(*exchanges[step])
    columns = []
    for pair in (sums[:2], sums[2:]):
        sent = jnp.concatenate([c.block(2, 1).astype(jnp.bfloat16) for c in pair], axis=1)
        came = swap(sent, "fs_0", 1)
        columns.append(added([jnp.concatenate([c.block(2, 0) for c in pair], axis=1), came]))
    mixed = jnp.concatenate(columns, axis=1).astype(jnp.bfloat16)[None]
    gate_t, up_t = assemble(where, sides)
    return (jnp.swapaxes(gate_t, 1, 2), jnp.swapaxes(up_t, 1, 2), down_out, mixed)


def solution(mesh):
    split = Mesh(
        mesh.devices.reshape(mesh.shape["gr"], 2, 4, 4, mesh.shape["tp"]),
        ("gr", "fs_0", "fs_1", "fs_2", "tp"),
    )
    in_specs = (
        P(("gr", "tp"), None, None),
        P(None, FS, ("gr", "tp")),
        P(None, FS, ("gr", "tp")),
        P(None, FS, ("gr", "tp")),
        P(FS),
        P(("gr", "tp"), None, None),
        P(("gr", "tp"), None, None),
    )
    out_specs = (P(None, None, FS), P(None, None, FS), P(None, FS, None), P(("gr", "tp"), FS, None))
    return jax.shard_map(
        program, mesh=split, in_specs=in_specs, out_specs=out_specs, check_vma=False
    )
```

```python
import jax
import jax.numpy as jnp
from jax import lax
from jax.experimental import pallas as pl
from jax.experimental.pallas import tpu as pltpu
from jax.sharding import Mesh
from jax.sharding import PartitionSpec as P

FS = ("fs_0", "fs_1", "fs_2")
PLANE = ("fs_1", "fs_2")
Z = ("gr", "fs_0")
UNITS = 256
MIB = 1024 * 1024
LAST_VMEM = 32


COLORS = (
    ((1, 1), (1, 3), (2, 1), (2, 3)),
    ((2, 1), (2, 3), (1, 1), (1, 3)),
    ((1, 3), (1, 1), (2, 3), (2, 1)),
    ((2, 3), (2, 1), (1, 3), (1, 1)),
)


def call(kernel, grid, ins, outs, out_shape, args, flops, nbytes, scratch=(), vmem=60):
    return pl.pallas_call(
        kernel,
        out_shape=out_shape,
        grid_spec=pltpu.PrefetchScalarGridSpec(
            num_scalar_prefetch=1,
            grid=grid,
            in_specs=ins,
            out_specs=outs,
            scratch_shapes=list(scratch),
        ),
        compiler_params=pltpu.CompilerParams(vmem_limit_bytes=vmem * MIB),
        cost_estimate=pl.CostEstimate(
            flops=int(flops), bytes_accessed=int(nbytes), transcendentals=0
        ),
    )(*args)


def whole(shape):
    return pl.BlockSpec(shape, lambda *_: (0,) * len(shape))


def shaped(*shape, dtype=jnp.bfloat16):
    return jax.ShapeDtypeStruct(shape, dtype)


def pack_kernel(where_ref, gate_ref, up_ref, gain_ref, own_ref, send_ref):
    depth = gain_ref.shape[1]
    gain = jnp.broadcast_to(gain_ref[...], (128, depth)).T[:, :1]
    rows = jnp.concatenate([gate_ref[0] * gain, up_ref[0] * gain], axis=0)
    cols = rows.astype(jnp.bfloat16).T
    dests, _, half, lanes = own_ref.shape
    cols = cols.reshape(dests, 2, half, lanes)
    low, high = cols[:, 0], cols[:, 1]
    first = where_ref[1] == 0
    own_ref[:, 0] = jnp.where(first, low, high)
    send_ref[:, 0] = jnp.where(first, high, low)


def pack(where, gate, up, gain, dests):
    experts, depth, width = gate.shape
    half = width // dests // 2
    block = pl.BlockSpec((1, depth, width), lambda e, w: (e, 0, 0))
    out = pl.BlockSpec((dests, 1, half, 2 * depth), lambda e, w: (0, e, 0, 0))
    return call(
        pack_kernel, (experts,), [block, block, whole((1, depth))], [out] * 2,
        [shaped(dests, experts, half, 2 * depth)] * 2, (where, gate, up, gain), 3e9, 6e6,
    )


def unpack_kernel(where_ref, own_ref, down_ref, up_ref, far_ref, out_ref):
    z = where_ref[0]
    sources, half, lanes = own_ref.shape
    left = lax.broadcasted_iota(jnp.int32, (half, lanes), 1) < lanes // 2
    pick = ((own_ref, down_ref, far_ref, up_ref), (down_ref, far_ref, up_ref, own_ref))
    for plane in range(4):

        @pl.when(z == plane)
        def _():
            for part in range(2):
                ref = pick[part][plane]
                for pair in range(sources // 2):
                    one = ref[2 * pair].astype(jnp.float32)
                    other = ref[2 * pair + 1].astype(jnp.float32)
                    crossed = pltpu.roll(jnp.where(left, other, one), lanes // 2, 1)
                    start = part * sources * (lanes // 2) + pair * lanes
                    at = slice(start, start + lanes)
                    out_ref[0, :, at] = jnp.where(left, one, crossed).astype(jnp.bfloat16)
                    out_ref[1, :, at] = jnp.where(left, crossed, other).astype(jnp.bfloat16)


def unpack(where, pieces):
    sources, half, lanes = pieces[0].shape
    shape = (2, half, sources * lanes)
    return call(
        unpack_kernel, (1,), [whole(pieces[0].shape)] * 4, whole(shape),
        shaped(*shape), (where, *pieces), 1e9, 3e6, vmem=12,
    )


def assemble_kernel(where_ref, *refs):
    gate_ref, up_ref = refs[-2:]
    tp = where_ref[1]
    half = refs[0].shape[1]
    for index, ref in enumerate(refs[:-2]):
        side = tp if index % 2 == 0 else 1 - tp
        rows = pl.ds(pl.multiple_of(side * half, 16), half)
        gate_ref[index // 2, rows, :] = ref[0]
        up_ref[index // 2, rows, :] = ref[1]


def assemble(where, sides):
    _, half, width = sides[0].shape
    shape = (len(sides) // 2, 2 * half, width)
    return call(
        assemble_kernel, (1,), [whole(sides[0].shape)] * len(sides),
        [whole(shape)] * 2, [shaped(*shape)] * 2, (where, *sides), 4e9, 11e6, vmem=26,
    )


def join_kernel(where_ref, *refs):
    out_ref, padded_ref = refs[-2:]
    tp, gr = where_ref[1], where_ref[2]
    depth, width = refs[0].shape[1:]
    places = (gr * 2 + tp, (1 - gr) * 2 + tp, gr * 2 + 1 - tp, (1 - gr) * 2 + 1 - tp)
    for ref, place in zip(refs[:-2], places):
        at = pl.ds(pl.multiple_of(place * width, width), width)
        out_ref[0, :, at] = ref[0]
        padded_ref[0, :depth, at] = ref[0]
    rest = padded_ref.shape[1] - depth
    padded_ref[0, depth:, :] = jnp.zeros((rest, padded_ref.shape[2]), jnp.bfloat16)


def join(where, quarters):
    experts, depth, width = quarters[0].shape
    at = lambda e, w: (e, 0, 0)
    return call(
        join_kernel, (experts,), [pl.BlockSpec((1, depth, width), at)] * 4,
        [pl.BlockSpec((1, depth, 4 * width), at), pl.BlockSpec((1, UNITS, 4 * width), at)],
        [shaped(experts, depth, 4 * width), shaped(experts, UNITS, 4 * width)],
        (where, *quarters), 2e9, 8e6, vmem=16,
    )


def norm_kernel(where_ref, tokens_ref, mix_ref, out_ref, mix_out_ref):
    z, x = where_ref[0] % 2, where_ref[4]
    rows = tokens_ref.shape[3]
    for place in range(8):
        zz, xx = z ^ (place % 2), x ^ (place // 2)
        values = tokens_ref[zz, 0, xx].astype(jnp.float32)
        scale = lax.rsqrt(jnp.mean(values * values, axis=-1, keepdims=True) + 1e-06)
        at = slice(place * rows, (place + 1) * rows)
        out_ref[0, at, :] = (values * scale).astype(jnp.bfloat16)
        mix_out_ref[0, at, :] = mix_ref[zz, 0, xx]


def norm(where, tokens, mix):
    zs, ys, xs, rows, width = tokens.shape
    experts = mix.shape[-1]
    block = lambda last: pl.BlockSpec((zs, 1, xs, rows, last), lambda i, w: (0, w[3] ^ i, 0, 0, 0))
    out = lambda last: pl.BlockSpec((1, xs * zs * rows, last), lambda i, w: (i, 0, 0))
    return call(
        norm_kernel, (ys,), [block(width), block(experts)], [out(width), out(experts)],
        [
            shaped(ys, xs * zs * rows, width),
            shaped(ys, xs * zs * rows, experts, dtype=jnp.float32),
        ],
        (where, tokens, mix), 6e9, 17e6,
    )


def fill(where_ref, own_ref, other_ref, gate, up):
    tp = where_ref[1]
    half = own_ref.shape[1]
    for ref, side in ((own_ref, tp), (other_ref, 1 - tp)):
        rows = pl.ds(pl.multiple_of(side * half, 16), half)
        gate[rows, :] = ref[0]
        up[rows, :] = ref[1]
    rest = jnp.zeros((gate.shape[0] - 2 * half, gate.shape[1]), jnp.bfloat16)
    gate[2 * half :, :] = rest
    up[2 * half :, :] = rest


def hidden_of(normed, mix, gate, up):
    dims = (((1,), (1,)), ((), ()))
    gate_act = lax.dot_general(normed, gate, dims, preferred_element_type=jnp.float32)
    up_act = lax.dot_general(normed, up, dims, preferred_element_type=jnp.float32)
    return (gate_act / (1.0 + jnp.exp(-gate_act)) * up_act * mix).astype(jnp.bfloat16)


def hidden_kernel(expert, where_ref, normed_ref, mix_ref, own_ref, other_ref, out_ref, gate, up):
    @pl.when(pl.program_id(0) == 0)
    def _():
        fill(where_ref, own_ref, other_ref, gate, up)

    mix = mix_ref[0, :, expert : expert + 1]
    out_ref[0] = hidden_of(normed_ref[0], mix, gate[...], up[...])


def hidden_units(where, normed, mix, own, other, expert):
    groups, rows, width = normed.shape
    at = lambda g, w: (g, 0, 0)
    side = whole(own.shape)
    weight = pltpu.VMEM((UNITS, width), jnp.bfloat16)
    return call(
        lambda *refs: hidden_kernel(expert, *refs), (groups,),
        [pl.BlockSpec((1, rows, width), at), pl.BlockSpec((1, rows, mix.shape[-1]), at), side, side],
        pl.BlockSpec((1, rows, UNITS), at), shaped(groups, rows, UNITS),
        (where, normed, mix, own, other), 4 * groups * rows * width * UNITS, 12e6,
        scratch=(weight, weight), vmem=48,
    )


def last_kernel(where_ref, normed_ref, mix_ref, early_ref, *refs):
    sides, down_ref = (refs[0:2], refs[2:4]), refs[4]
    outs, weights = refs[5:-4], (refs[-4:-2], refs[-2:])
    yy = pl.program_id(0)

    @pl.when(yy == 0)
    def _():
        for side, weight in zip(sides, weights):
            fill(where_ref, *side, *weight)

    hidden = [early_ref[0]]
    for expert, (gate, up) in enumerate(weights, 1):
        mix = mix_ref[0, :, expert : expert + 1]
        hidden.append(hidden_of(normed_ref[0], mix, gate[...], up[...]))
    rows = jnp.concatenate(hidden, axis=1)
    block = rows.shape[0]
    ys = pl.num_programs(0)
    width = outs[0].shape[1]
    for color, exchanges in enumerate(COLORS):
        at = slice(color * width, (color + 1) * width)
        product = jnp.dot(rows, down_ref[:, at], preferred_element_type=jnp.float32)
        product = product.astype(jnp.bfloat16)
        send_ref, keep_refs = outs[3 * color], outs[3 * color + 1 : 3 * color + 3]
        axis, mask = exchanges[0]
        if axis == 1:
            for at_y, ref, start in (
                (0, keep_refs[0], 0),
                (4 - mask, keep_refs[1], 0),
                (mask, send_ref, 0),
                (2, send_ref, block),
            ):

                @pl.when(yy == at_y)
                def _():
                    ref[start : start + block, :] = product

        else:
            part = block // 4
            for xx, ref, k in (
                (0, keep_refs[0], 0),
                (4 - mask, keep_refs[1], 0),
                (mask, send_ref, 0),
                (2, send_ref, 1),
            ):
                to = pl.ds(pl.multiple_of((k * ys + yy) * part, part), part)
                ref[to, :] = product[xx * part : (xx + 1) * part]


def last(where, normed, mix, early, sides, down):
    ys, rows, width = normed.shape
    quarter = (ys * rows // 4, width // len(COLORS))
    outs = [(2 * quarter[0], quarter[1]), quarter, quarter] * len(COLORS)
    at = lambda i, w: (i, 0, 0)
    side = whole(sides[0].shape)
    weight = pltpu.VMEM((UNITS, width), jnp.bfloat16)
    return call(
        last_kernel, (ys,),
        [pl.BlockSpec((1, rows, width), at), pl.BlockSpec((1, rows, mix.shape[-1]), at)]
        + [pl.BlockSpec((1, rows, UNITS), at)] + [side] * 4 + [whole(down.shape)],
        [whole(out) for out in outs], [shaped(*out) for out in outs],
        (where, normed, mix, early, *sides, down), 14 * ys * rows * width * UNITS, 25e6,
        scratch=(weight,) * 4, vmem=LAST_VMEM,
    )


def swap(array, axis, mask):
    peers = lax.axis_size(axis)
    return lax.ppermute(array, axis, [(i, i ^ mask) for i in range(peers)])


def added(terms):
    total = terms[0].astype(jnp.float32)
    for term in terms[1:]:
        total = total + term.astype(jnp.float32)
    return total


class Sums:
    def __init__(self, send, keeps, exchanges):
        axis, mask = exchanges[0]
        self.axes = (axis, *(a for a in (1, 2, 0) if a != axis))
        sizes = [2 if a == 0 else 4 for a in self.axes]
        sizes[0] //= 2
        shape = (*sizes, -1, send.shape[-1])
        came = swap(send, FS[axis], mask).reshape(shape)
        self.offsets = [[0, 1, 2, 3] if a else [0, 1] for a in self.axes]
        self.offsets[0] = [0, 4 - mask] if axis else [0]
        places = [list(range(size)) for size in sizes]
        keeps = [keep.reshape(1, *shape[1:]) for keep in keeps]
        self.terms = [(keeps, places), (came, [list(p) for p in places])]

    def at(self, dim, index):
        parts = []
        for array, places in self.terms:
            for d, place in enumerate(places):
                if isinstance(array, list):
                    array = array[place[index if dim == 0 else 0]]
                elif d == dim:
                    array = lax.slice_in_dim(array, place[index], place[index] + 1, axis=d)
                elif len(place) < array.shape[d]:
                    array = lax.slice_in_dim(array, place[0], place[0] + 1, axis=d)
            parts.append(array)
        return added(parts)

    def exchange(self, axis, mask):
        dim = self.axes.index(axis)
        have = self.offsets[dim]
        going, staying = ([mask], [0]) if len(have) == 2 else ([mask, 2], [0, 4 - mask])
        send = [self.at(dim, have.index(o)).astype(jnp.bfloat16) for o in going]
        came = swap(jnp.concatenate(send, axis=dim), FS[axis], mask)
        for _, places in self.terms:
            places[dim] = [places[dim][have.index(o)] for o in staying]
        self.terms.append((came, [list(range(size)) for size in came.shape[:3]]))
        self.offsets[dim] = staying

    def block(self, dim, index):
        total = self.at(dim, index)
        return total.reshape(total.shape[-2:])


def mixing(chosen, weights, experts):
    share = weights / jnp.sum(weights, axis=-1, keepdims=True)
    labels = jnp.arange(experts, dtype=jnp.int32)
    match = (chosen[:, :, None] == labels[None, None, :]).astype(jnp.float32)
    return jnp.sum(share[:, :, None] * match, axis=1)


def program(tokens, gate_master, up_master, down_master, norm_gain, route, route_weight):
    z, tp = lax.axis_index(Z), lax.axis_index("tp")
    where = [z, tp, lax.axis_index("gr"), lax.axis_index("fs_1"), lax.axis_index("fs_2")]
    where = jnp.stack(where).astype(jnp.int32)
    experts = gate_master.shape[0]
    peers = lax.axis_size(PLANE)
    other_core = lambda v: swap(v, "tp", 1)
    gain = norm_gain[None, :]

    own, send = pack(where, gate_master, up_master, gain, peers // 2)
    came = other_core(send)
    blocks = jnp.where(
        tp == 0, jnp.concatenate([own, came], axis=0), jnp.concatenate([came, own], axis=0)
    )
    combine = mixing(route[0], route_weight[0], experts)
    blocks, combine = lax.optimization_barrier((blocks, combine))
    mine = lax.all_to_all(blocks, PLANE, split_axis=0, concat_axis=0, tiled=True)

    down_own = down_master.astype(jnp.bfloat16)
    down_far = swap(down_own, "gr", 1)
    down_own_core, down_far_core = other_core(down_own), other_core(down_far)

    _, width = tokens.shape[1:]
    places = [lax.axis_size(a) for a in FS]
    normed, mix = norm(
        where, tokens.reshape(*places, -1, width), combine.reshape(*places, -1, experts)
    )
    quarters = (down_own, down_far, down_own_core, down_far_core)
    down_out, down_padded = join(where, quarters)
    mine, normed = lax.optimization_barrier((mine, normed))

    sides = []
    for e in range(experts):
        piece = mine[:, e]
        below = lax.ppermute(piece, Z, [(1, 0), (2, 1), (0, 3)])
        above = lax.ppermute(piece, Z, [(1, 2), (2, 3), (3, 0)])
        passed = jnp.where(z == 3, below, above)
        far = lax.ppermute(passed, Z, [(3, 2), (0, 1)])
        own = unpack(where, (piece, below, above, far))
        sides += [own, other_core(own)]
    early = hidden_units(where, normed, mix, sides[0], sides[1], 0)
    outs = last(where, normed, mix, early, sides[2:], down_padded.reshape(-1, width))
    sums = []
    for color, exchanges in enumerate(COLORS):
        sums.append(Sums(outs[3 * color], outs[3 * color + 1 : 3 * color + 3], exchanges))
    for step in range(1, 4):
        for color, exchanges in zip(sums, COLORS):
            color.exchange(*exchanges[step])
    columns = []
    for pair in (sums[:2], sums[2:]):
        sent = jnp.concatenate([c.block(2, 1).astype(jnp.bfloat16) for c in pair], axis=1)
        came = swap(sent, "fs_0", 1)
        columns.append(added([jnp.concatenate([c.block(2, 0) for c in pair], axis=1), came]))
    mixed = jnp.concatenate(columns, axis=1).astype(jnp.bfloat16)[None]
    gate_t, up_t = assemble(where, sides)
    return (jnp.swapaxes(gate_t, 1, 2), jnp.swapaxes(up_t, 1, 2), down_out, mixed)


def solution(mesh):
    split = Mesh(
        mesh.devices.reshape(mesh.shape["gr"], 2, 4, 4, mesh.shape["tp"]),
        ("gr", "fs_0", "fs_1", "fs_2", "tp"),
    )
    in_specs = (
        P(("gr", "tp"), None, None),
        P(None, FS, ("gr", "tp")),
        P(None, FS, ("gr", "tp")),
        P(None, FS, ("gr", "tp")),
        P(FS),
        P(("gr", "tp"), None, None),
        P(("gr", "tp"), None, None),
    )
    out_specs = (P(None, None, FS), P(None, None, FS), P(None, FS, None), P(("gr", "tp"), FS, None))
    return jax.shard_map(
        program, mesh=split, in_specs=in_specs, out_specs=out_specs, check_vma=False
    )
```
